32 devices in a mesh: grp: 2 (over y), sp: 4 (over z), tp: 4 (over x, core).
Axes of the slice: x: 2, y: 2, z: 4, core: 2. Of those that a mesh axis runs over, the one named last changes fastest.
Arguments:
- input_wide: bfloat16 [1024, 512], P(('grp', 'sp'), 'tp'), parts along dimension 0, may hold values from -6 to 6
- input_narrow: bfloat16 [1024, 512], P(('grp', 'sp'), 'tp'), parts along dimension 0, may hold values from -6 to 6
- spacing: float32 [1024], P(('grp', 'sp')), parts along dimension 0, may hold values from 0.2 to 208
- rate_wide: float32 [2, 32, 64], P(None, 'tp'), may hold values from 0.0009765625 to 0.035
- turn_wide: float32 [2, 32, 64], P(None, 'tp'), may hold values from 0.1 to 1.5
- drive_wide: float32 [2, 32, 16, 128], P(None, 'tp'), may hold values from -0.2 to 0.2
- read_wide: float32 [2, 32, 16, 128], P(None, 'tp'), may hold values from -0.5 to 0.5
- narrow_decay_rate: float32 [2, 32, 32], P(None, 'tp'), may hold values from 0.0009765625 to 0.035
- turn_narrow: float32 [2, 32, 32], P(None, 'tp'), may hold values from 0.1 to 1.5
- drive_narrow: float32 [2, 32, 16, 64], P(None, 'tp'), may hold values from -0.2 to 0.2
- read_narrow: float32 [2, 32, 16, 64], P(None, 'tp'), may hold values from -0.75 to 0.75
- skip_gain: float32 [2, 512], P(None, 'tp'), may hold values from -4 to 4
- out_value: bfloat16 [1024, 1024], P(None, 'tp'), may hold values from -0.1875 to 0.1875
- out_gate: bfloat16 [1024, 1024], P(None, 'tp'), may hold values from -0.1875 to 0.1875
- stream: bfloat16 [1024, 1024], P(('grp', 'sp'), 'tp'), parts along dimension 0, may hold values from -20 to 20
- norm_gain: float32 [1024], P('tp'), may hold values from 0.1 to 1.9
- up_value: bfloat16 [1024, 5632], P('sp', 'tp'), may hold values from -0.1875 to 0.1875
- up_gate: bfloat16 [1024, 5632], P('sp', 'tp'), may hold values from -0.1875 to 0.1875
- conv_taps: float32 [2, 3, 5632], P(None, None, 'tp'), may hold values from -3.5 to 3.5
- down_weight: bfloat16 [5632, 1024], P('tp', 'sp'), may hold values from -0.078125 to 0.078125
Outputs:
- mixed: bfloat16 [1024, 1024], P(('grp', 'sp'), 'tp'), parts along dimension 0
The draws below stay inside these ranges and needn't reach their ends.
There are 2 independent parts, one for each index of `grp`. The reference program is written for one: setup_inputs(seed, part) draws one part's arguments, and reference() takes and returns one part's arrays. A program takes and returns all parts, laid end to end along the dimension named above; an argument that names none is the same for every part. Nothing has to cross between parts.
All inputs are finite; a program needn't handle non-finite values.
Results may differ from the reference program's by a relative error of at most 0.017.
Values may be sent and summed in bfloat16 or wider, within the bound.
A program may use at most 128 MiB of HBM per device.

```python
import math
import jax
import jax.numpy as jnp
from jax import lax

DA = 512
DB = 512
GROUP = 16
PA = 64
PB = 32
FF = 5632
TOK_DEV = 128
D = 1024
SEQUENCE_SLOTS = 512
N_TP = 4


def rates_and_drive(key, groups, states):
    keys = jax.random.split(key, 4)
    share = 0.5
    quick = jax.random.bernoulli(keys[0], share, (2, groups, 1))
    slow_floor = 0.5 / SEQUENCE_SLOTS
    slow = slow_floor * jnp.exp(jax.random.uniform(keys[1], (2, groups, states), jnp.float32, 0.0, math.log(2.0)))
    fast = 0.01 * jnp.exp(jax.random.uniform(keys[2], (2, groups, states), jnp.float32, 0.0, math.log(3.5)))
    rate = jnp.where(quick, fast, slow)
    scale = jnp.sqrt(2.0 * rate / (2.0 * GROUP))
    scale = jnp.concatenate([scale, scale], axis=-1)[:, :, None, :]
    drive = jnp.clip(jax.random.normal(keys[3], (2, groups, GROUP, 2 * states), jnp.float32), -4.0, 4.0) * scale
    return (rate, drive)


def draw_rate_wide(key, part):
    return rates_and_drive(jax.random.fold_in(key, 11), DA // GROUP, PA)[0]


def draw_drive_wide(key, part):
    return rates_and_drive(jax.random.fold_in(key, 11), DA // GROUP, PA)[1]


def draw_narrow_decay_rate(key, part):
    return rates_and_drive(jax.random.fold_in(key, 23), DB // GROUP, PB)[0]


def draw_drive_narrow(key, part):
    return rates_and_drive(jax.random.fold_in(key, 23), DB // GROUP, PB)[1]


def draw_spacing(key, part):
    keys = jax.random.split(key, 3)
    blocks = SEQUENCE_SLOTS // TOK_DEV
    level = jnp.exp(jax.random.uniform(keys[0], (blocks,), jnp.float32, -0.69, 0.69))
    rough = jax.random.uniform(keys[1], (SEQUENCE_SLOTS,), jnp.float32, 0.5, 1.5)
    starting_shift = jnp.repeat(level, TOK_DEV) * rough
    slot_number = jax.random.randint(keys[2], (3,), 0, SEQUENCE_SLOTS)
    pulse_source = jnp.zeros((SEQUENCE_SLOTS,), jnp.float32).at[slot_number].set(0.4 * SEQUENCE_SLOTS)
    return starting_shift + pulse_source


def draw_stream(key, part):
    keys = jax.random.split(key, 2)
    values = jnp.clip(jax.random.normal(keys[0], (SEQUENCE_SLOTS, D), jnp.float32), -4.0, 4.0)
    rows = 10.0 ** jax.random.uniform(keys[1], (SEQUENCE_SLOTS, 1), jnp.float32, -0.5, 0.5)
    columns = 10.0 ** jnp.linspace(-0.5, 0.5, D, dtype=jnp.float32)
    return (values * rows * columns[None, :] * 0.5).astype(jnp.bfloat16)


def shard_levels(stream_key, shape, cuts, least, largest):
    loudness = 1.0
    for position, parts in cuts:
        heights = jax.random.uniform(jax.random.fold_in(jax.random.fold_in(stream_key, 6), position), (parts,), jnp.float32, least / len(cuts), largest / len(cuts))
        loudness = loudness * jnp.repeat(jnp.exp(heights), shape[position] // parts).reshape((-1,) + (1,) * (len(shape) - 1 - position))
    return loudness


def normal_values(stream_key, shape, deviation, limit, cuts=(), held_as=jnp.bfloat16):
    level = shard_levels(stream_key, shape, cuts, -0.22, 0.18) if cuts else 1.0
    values = jax.random.normal(stream_key, shape, jnp.float32) * deviation * level
    return jnp.minimum(jnp.maximum(values, -limit), limit).astype(held_as)


def setup_inputs(seed: int = 0, part: int = 0) -> dict:
    key_list = jax.random.split(jax.random.key(seed), 21)
    own_keys = jax.random.split(jax.random.fold_in(key_list[20], part), 21)
    input_wide = normal_values(own_keys[0], (SEQUENCE_SLOTS, DA), 1.0, 6.0, ((0, 4), (1, 4)))
    input_narrow = normal_values(own_keys[1], (SEQUENCE_SLOTS, DB), 1.0, 6.0, ((0, 4), (1, 4)))
    spacing = draw_spacing(jax.random.fold_in(jax.random.fold_in(key_list[20], part), 71), part)
    rate_wide = draw_rate_wide(jax.random.fold_in(key_list[20], 71), part)
    turn_wide = jnp.clip(0.1 + 1.4 * jax.random.uniform(key_list[4], (2, DA // GROUP, PA), jnp.float32) ** shard_levels(key_list[4], (2, DA // GROUP, PA), ((1, 4),), -0.2, 0.2), 0.1, 1.5)
    drive_wide = draw_drive_wide(jax.random.fold_in(key_list[20], 71), part)
    read_wide = normal_values(key_list[6], (2, DA // GROUP, GROUP, 2 * PA), (2 * PA) ** -0.5, 0.5, ((1, 4),), jnp.float32)
    narrow_decay_rate = draw_narrow_decay_rate(jax.random.fold_in(key_list[20], 71), part)
    turn_narrow = jnp.clip(0.1 + 1.4 * jax.random.uniform(key_list[8], (2, DB // GROUP, PB), jnp.float32) ** shard_levels(key_list[8], (2, DB // GROUP, PB), ((1, 4),), -0.2, 0.2), 0.1, 1.5)
    drive_narrow = draw_drive_narrow(jax.random.fold_in(key_list[20], 71), part)
    read_narrow = normal_values(key_list[10], (2, DB // GROUP, GROUP, 2 * PB), (2 * PB) ** -0.5, 0.75, ((1, 4),), jnp.float32)
    skip_gain = normal_values(key_list[11], (2, DA), 1.0, 4.0, ((1, 4),), jnp.float32)
    out_value = normal_values(key_list[12], (D, D), D ** -0.5, 0.1875, ((1, 4),))
    out_gate = normal_values(key_list[13], (D, D), D ** -0.5, 0.1875, ((1, 4),))
    stream = draw_stream(jax.random.fold_in(jax.random.fold_in(key_list[20], part), 71), part)
    norm_gain = jnp.clip(1.0 + 0.18 * jax.random.normal(key_list[15], (D,), jnp.float32), 0.1, 1.9)
    up_value = normal_values(key_list[16], (D, FF), D ** -0.5, 0.1875, ((0, 4), (1, 4)))
    up_gate = normal_values(key_list[17], (D, FF), D ** -0.5, 0.1875, ((0, 4), (1, 4)))
    conv_taps = normal_values(key_list[18], (2, 3, FF), 3 ** -0.5, 3.5, ((2, 4),), jnp.float32)
    down_weight = normal_values(key_list[19], (FF, D), FF ** -0.5, 0.078125, ((0, 4), (1, 4)))
    return {"input_wide": input_wide, "input_narrow": input_narrow, "spacing": spacing, "rate_wide": rate_wide, "turn_wide": turn_wide, "drive_wide": drive_wide, "read_wide": read_wide, "narrow_decay_rate": narrow_decay_rate, "turn_narrow": turn_narrow, "drive_narrow": drive_narrow, "read_narrow": read_narrow, "skip_gain": skip_gain, "out_value": out_value, "out_gate": out_gate, "stream": stream, "norm_gain": norm_gain, "up_value": up_value, "up_gate": up_gate, "conv_taps": conv_taps, "down_weight": down_weight}


precise = lax.Precision.HIGHEST
epsilon = 1e-06

def complex_times(left_real, left_quad, right_real, right_quad):
    return (left_real * right_real - left_quad * right_quad, left_real * right_quad + left_quad * right_real)

def step_factors(rate, turn, spacing):
    shrink = jnp.exp(-rate * spacing)
    angle = turn * spacing
    decay_real = shrink * jnp.cos(angle)
    decay_quad = shrink * jnp.sin(angle)
    square = rate * rate + turn * turn
    coef_real, coef_quad = complex_times(decay_real - 1.0, decay_quad, -rate / square, -turn / square)
    return (decay_real, decay_quad, coef_real, coef_quad)

def state_pass(inputs, spacing, rate, turn, drive, read, reverse):
    extent = inputs.shape[0]
    groups = rate.shape[0]
    states = rate.shape[1]
    clustered = inputs.astype(jnp.float32).reshape(extent, groups, GROUP)

    def advance(carry, item):
        state_real, state_quad = carry
        values, spot = item
        decay_real, decay_quad, coef_real, coef_quad = step_factors(rate, turn, spot)
        pushed = jnp.einsum('gc,gcq->gq', values, drive, precision=precise)
        kick_real, impulse_quadrature = complex_times(coef_real, coef_quad, pushed[:, :states], pushed[:, states:])
        kept_real, kept_quad = complex_times(decay_real, decay_quad, state_real, state_quad)
        state_real = kept_real + kick_real
        state_quad = kept_quad + impulse_quadrature
        joined = jnp.concatenate([state_real, state_quad], axis=1)
        reading = jnp.einsum('gq,gcq->gc', joined, read, precision=precise)
        return ((state_real, state_quad), reading)
    start = (jnp.zeros((groups, states), jnp.float32), jnp.zeros((groups, states), jnp.float32))
    _, readings = lax.scan(advance, start, (clustered, spacing), reverse=reverse)
    return readings.reshape(extent, groups * GROUP)

def mixer_half(inputs, spacing, rate, turn, drive, read, skip):
    reading = state_pass(inputs, spacing, rate[0], turn[0], drive[0], read[0], False)
    reading = reading + state_pass(inputs, spacing, rate[1], turn[1], drive[1], read[1], True)
    return jax.nn.gelu(reading + skip * inputs.astype(jnp.float32)).astype(jnp.bfloat16)

def reference(input_wide, input_narrow, spacing, rate_wide, turn_wide, drive_wide, read_wide, narrow_decay_rate, turn_narrow, drive_narrow, read_narrow, skip_gain, out_value, out_gate, stream, norm_gain, up_value, up_gate, conv_taps, down_weight):
    mixer_in = jnp.concatenate([mixer_half(input_wide, spacing, rate_wide, turn_wide, drive_wide, read_wide, skip_gain[0]), mixer_half(input_narrow, spacing, narrow_decay_rate, turn_narrow, drive_narrow, read_narrow, skip_gain[1])], axis=1)
    value = jnp.dot(mixer_in, out_value, preferred_element_type=jnp.float32)
    gate = jnp.dot(mixer_in, out_gate, preferred_element_type=jnp.float32)
    middle = (stream.astype(jnp.float32) + value * jax.nn.sigmoid(gate)).astype(jnp.bfloat16)
    expanded_width = middle.astype(jnp.float32)
    scale = lax.rsqrt(lax.optimization_barrier(jnp.mean(expanded_width * expanded_width, axis=1, keepdims=True)) + epsilon)
    normed = (expanded_width * scale * norm_gain).astype(jnp.bfloat16)
    pre = jnp.concatenate([jnp.dot(normed, up_value, preferred_element_type=jnp.float32), jnp.dot(normed, up_gate, preferred_element_type=jnp.float32)], axis=1).astype(jnp.bfloat16)
    padded = jnp.pad(pre, ((1, 1), (0, 0)))
    taps = jnp.concatenate([conv_taps[0], conv_taps[1]], axis=1)
    conv = taps[0] * padded[:-2] + taps[1] * padded[1:-1] + taps[2] * padded[2:]
    hidden = (jax.nn.silu(conv[:, FF:]) * conv[:, :FF]).astype(jnp.bfloat16)
    block = FF // N_TP
    ffn = jnp.zeros((hidden.shape[0], down_weight.shape[1]), jnp.float32)
    for index in range(N_TP):
        partial_value = jnp.dot(hidden[:, index * block:(index + 1) * block], down_weight[index * block:(index + 1) * block], preferred_element_type=jnp.float32)
        ffn = ffn + lax.optimization_barrier(partial_value.astype(jnp.bfloat16)).astype(jnp.float32)
    return (middle.astype(jnp.float32) + ffn).astype(jnp.bfloat16)
```

```python
import functools

import jax
import jax.numpy as jnp
from jax import lax
from jax.experimental import pallas as pl
from jax.experimental.pallas import tpu as pltpu
from jax.sharding import PartitionSpec as P

GROUP = 16
LANES = 128
epsilon = 1e-06
f32 = jnp.float32
bf16 = jnp.bfloat16


def sin_cos(angle):
    turns = jnp.round(angle * 0.6366197723675814)
    r = angle - turns * 1.5703125
    r = r - turns * 4.837512969970703125e-4
    r = r - turns * 7.54978995489188216e-8
    z = r * r
    s = ((-1.9515295891e-4 * z + 8.3321608736e-3) * z - 1.6666654611e-1) * z * r + r
    c = ((2.443315711809948e-5 * z - 1.388731625493765e-3) * z + 4.166664568298827e-2) * z * z - 0.5 * z + 1.0
    quadrant = turns.astype(jnp.int32)
    odd = (quadrant & 1) == 1
    sin = jnp.where(odd, c, s)
    cos = jnp.where(odd, s, c)
    sin = jnp.where((quadrant & 2) == 2, -sin, sin)
    cos = jnp.where(((quadrant + 1) & 2) == 2, -cos, cos)
    return sin, cos


def decay_of(rate, turn, span):
    shrink = jnp.exp(-rate * span)
    sin, cos = sin_cos(turn * span)
    return shrink * cos, shrink * sin


def times(ar, ai, br, bi):
    return ar * br - ai * bi, ar * bi + ai * br


def split(value):
    high = value.astype(bf16)
    return high, (value - high.astype(f32)).astype(bf16)


def dot(a, b):
    return jnp.dot(a, b, preferred_element_type=f32)


def dot_nt(a, b):
    return lax.dot_general(a, b, (((1,), (1,)), ((), ())), preferred_element_type=f32)


def kernel(
    n, nt, starts,
    spacing, x_ref, rt_ref, drive_ref, read_ref, skip_ref, ov_ref, og_ref, stream_ref, gain_ref,
    taps_ref, upv_ref, upg_ref, down_ref,
    out_ref,
    upv, upg, down, kick, dec, ends, mix, mid, gain, pre, part, got, sums, done,
    w_send, w_recv, w_local, e_send, e_recv, g_send, g_recv, m_send, m_recv,
    z_send, z_recv, t_send, t_recv, p_send, p_recv, s_send, s_recv,
):
    me, mt = lax.axis_index("sp"), lax.axis_index("tp")
    tokens = x_ref.shape[0]
    groups = rt_ref.shape[2]
    channels = x_ref.shape[1] // 2
    width = upv.shape[1]
    rows = upv_ref.shape[0]
    cols = out_ref.shape[1]
    limit = upv_ref.shape[1] - width

    def remote(src, dst, send, recv, axis, peer):
        return pltpu.make_async_remote_copy(
            src_ref=src, dst_ref=dst, send_sem=send, recv_sem=recv,
            device_id={axis: peer}, device_id_type=pl.DeviceIdType.MESH)

    def start_of(index):
        return pl.multiple_of(jnp.minimum(index * width, limit), LANES)

    barrier = pltpu.get_barrier_semaphore()
    for offset in range(1, n):
        pl.semaphore_signal(barrier, inc=1, device_id={"sp": lax.rem(me + offset, n)},
                            device_id_type=pl.DeviceIdType.MESH)
    for offset in range(1, nt):
        pl.semaphore_signal(barrier, inc=1, device_id={"tp": lax.rem(mt + offset, nt)},
                            device_id_type=pl.DeviceIdType.MESH)
    pl.semaphore_wait(barrier, n + nt - 2)

    def weight_parts(which, target, slot):
        begin = start_of(target)
        place = pl.ds(pl.multiple_of(slot * rows, rows), rows)
        if which == 0:
            return upv_ref.at[:, pl.ds(begin, width)], upv.at[place, :]
        if which == 1:
            return upg_ref.at[:, pl.ds(begin, width)], upg.at[place, :]
        return (down_ref.at[pl.ds(begin, width), :],
                down.at[slot])

    def weight_copy(which, target, slot):
        src, dst = weight_parts(which, target, slot)
        return remote(src, dst, w_send.at[which, target], w_recv.at[which, slot], "sp", target)

    def weight_start(which):
        for offset in range(1, n):
            weight_copy(which, lax.rem(me + offset, n), me).start()

    def weight_wait(which):
        for offset in range(1, n):
            peer = lax.rem(me + offset, n)
            weight_copy(which, peer, me).wait_send()
            weight_copy(which, me, peer).wait_recv()
        src, dst = weight_parts(which, me, me)
        pltpu.make_async_copy(src, dst, w_local.at[which]).wait()

    for which in range(3):
        src, dst = weight_parts(which, me, me)
        pltpu.make_async_copy(src, dst, w_local.at[which]).start()

    def gain_copy(target, slot):
        return remote(gain_ref, gain.at[slot], g_send.at[target], g_recv.at[slot], "tp", target)

    for offset in range(1, nt):
        gain_copy(lax.rem(mt + offset, nt), mt).start()
    gain[mt] = gain_ref[...]

    x = x_ref[...]
    lane_group = lax.rem(lax.broadcasted_iota(jnp.int32, x.shape, 1), channels) // GROUP
    for d in range(2):
        high, low = split(drive_ref[d])
        for g in range(groups):
            picked = jnp.where(lane_group == g, x, jnp.zeros_like(x))
            pushed = dot(picked, high) + dot(picked, low)
            place = pl.ds(g, tokens, stride=groups)
            kick[d, 0, place, :] = pushed[:, :LANES]
            kick[d, 1, place, :] = pushed[:, LANES:]

    rates = [rt_ref[0, d] for d in range(2)]
    turns = [rt_ref[1, d] for d in range(2)]
    inverse = []
    for d in range(2):
        square = rates[d] * rates[d] + turns[d] * turns[d]
        inverse.append((-rates[d] / square, -turns[d] / square))

    def spot(d, i):
        return i if d == 0 else tokens - 1 - i

    def first(i, carry):
        state, total = list(carry[:4]), carry[4]
        for d in range(2):
            t = spot(d, i)
            step = spacing[t]
            if d == 0:
                total = total + step
            place = pl.ds(pl.multiple_of(t * groups, groups), groups)
            dr, di = decay_of(rates[d], turns[d], step)
            cr, ci = times(dr - 1.0, di, *inverse[d])
            kr, ki = times(cr, ci, kick[d, 0, place, :], kick[d, 1, place, :])
            dec[d, 0, place, :] = dr
            dec[d, 1, place, :] = di
            kick[d, 0, place, :] = kr
            kick[d, 1, place, :] = ki
            ar, ai = times(dr, di, state[2 * d], state[2 * d + 1])
            state[2 * d], state[2 * d + 1] = ar + kr, ai + ki
        return (*state, total)

    zero = jnp.zeros((groups, LANES), f32)
    found = lax.fori_loop(0, tokens, first, (zero, zero, zero, zero, jnp.float32(0.0)), unroll=4)
    for d in range(2):
        ar, ai = decay_of(rates[d], turns[d], found[4])
        ends[me, d, 0] = found[2 * d]
        ends[me, d, 1] = found[2 * d + 1]
        ends[me, d, 2] = ar
        ends[me, d, 3] = ai

    def ends_copy(target, slot):
        return remote(ends.at[slot], ends.at[slot], e_send.at[target], e_recv.at[slot], "sp", target)

    for offset in range(1, n):
        ends_copy(lax.rem(me + offset, n), me).start()
    weight_start(0)
    weight_start(1)
    for offset in range(1, n):
        peer = lax.rem(me + offset, n)
        ends_copy(peer, me).wait_send()
        ends_copy(me, peer).wait_recv()

    carry = []
    for d in range(2):
        cr, ci = zero, zero
        for k in range(n):
            s = k if d == 0 else n - 1 - k
            use = (s < me) if d == 0 else (s > me)
            nr, ni = times(ends[s, d, 2], ends[s, d, 3], cr, ci)
            flag = jnp.where(use, 1, 0)
            keep = jnp.full((groups, LANES), flag, jnp.int32) == 1
            cr = jnp.where(keep, nr + ends[s, d, 0], cr)
            ci = jnp.where(keep, ni + ends[s, d, 1], ci)
        carry += [cr, ci]

    def second(i, carry):
        state = list(carry)
        for d in range(2):
            t = spot(d, i)
            place = pl.ds(pl.multiple_of(t * groups, groups), groups)
            ar, ai = times(dec[d, 0, place, :], dec[d, 1, place, :], state[2 * d], state[2 * d + 1])
            state[2 * d] = ar + kick[d, 0, place, :]
            state[2 * d + 1] = ai + kick[d, 1, place, :]
            kick[d, 0, place, :] = state[2 * d]
            kick[d, 1, place, :] = state[2 * d + 1]
        return tuple(state)

    lax.fori_loop(0, tokens, second, tuple(carry), unroll=4)

    reading = skip_ref[...] * x.astype(f32)
    for d in range(2):
        high, low = split(read_ref[d])
        for g in range(groups):
            place = pl.ds(g, tokens, stride=groups)
            state = jnp.concatenate([kick[d, 0, place, :], kick[d, 1, place, :]], axis=1)
            state_high, state_low = split(state)
            value = dot_nt(state_high, high) + dot_nt(state_low, high) + dot_nt(state_high, low)
            reading = reading + jnp.where(lane_group == g, value, 0.0)
    mix[mt] = jax.nn.gelu(reading).astype(bf16)

    def mix_copy(target, slot):
        return remote(mix.at[slot], mix.at[slot], m_send.at[target], m_recv.at[slot], "tp", target)

    for offset in range(1, nt):
        mix_copy(lax.rem(mt + offset, nt), mt).start()
    for offset in range(1, nt):
        peer = lax.rem(mt + offset, nt)
        mix_copy(peer, mt).wait_send()
        mix_copy(mt, peer).wait_recv()

    value = jnp.zeros((tokens, cols), f32)
    gate = jnp.zeros((tokens, cols), f32)
    half = ov_ref.shape[0] // 2
    for k in range(nt):
        for h in range(2):
            piece = mix[k][:, h * channels:(h + 1) * channels]
            at = slice(h * half + k * channels, h * half + (k + 1) * channels)
            value = value + dot(piece, ov_ref[at, :])
            gate = gate + dot(piece, og_ref[at, :])
    mid[me, mt] = (stream_ref[...].astype(f32) + value * jax.nn.sigmoid(gate)).astype(bf16)

    def z_copy(target, slot):
        return remote(mid.at[slot, mt], mid.at[slot, mt], z_send.at[target], z_recv.at[slot], "sp", target)

    def t_copy(s, target, slot):
        return remote(mid.at[s, slot], mid.at[s, slot], t_send.at[s, target], t_recv.at[s, slot], "tp", target)

    for offset in range(1, n):
        z_copy(lax.rem(me + offset, n), me).start()
    for offset in range(1, nt):
        t_copy(me, lax.rem(mt + offset, nt), mt).start()
    weight_start(2)
    for offset in range(1, n):
        peer = lax.rem(me + n - offset, n) if offset % 2 else lax.rem(me + offset, n)
        peer = lax.rem(me + offset, n)
        z_copy(me, peer).wait_recv()
        for other in range(1, nt):
            t_copy(peer, lax.rem(mt + other, nt), mt).start()
    for offset in range(1, nt):
        peer = lax.rem(mt + offset, nt)
        gain_copy(peer, mt).wait_send()
        gain_copy(mt, peer).wait_recv()
    weight_wait(0)
    weight_wait(1)
    for offset in range(1, n):
        z_copy(lax.rem(me + offset, n), me).wait_send()

    for i in range(2):
        pre[pl.ds(i * (8 + n * tokens), 8), :] = jnp.zeros((8, 2 * width), f32)
    for step in range(n):
        s = lax.rem(me + step, n)
        for offset in range(1, nt):
            peer = lax.rem(mt + offset, nt)
            t_copy(s, peer, mt).wait_send()
            t_copy(s, mt, peer).wait_recv()
        squares = jnp.zeros((tokens, 1), f32)
        for k in range(nt):
            piece = mid[s, k].astype(f32)
            squares = squares + jnp.sum(piece * piece, axis=1, keepdims=True)
        scale = lax.rsqrt(squares / (nt * cols) + epsilon)
        normed = jnp.concatenate(
            [(mid[s, k].astype(f32) * scale * gain[k]).astype(bf16) for k in range(nt)], axis=1)
        place = pl.ds(pl.multiple_of(8 + s * tokens, 8), tokens)
        pre[place, :width] = dot(normed, upv[...]).astype(bf16).astype(f32)
        pre[place, width:] = dot(normed, upg[...]).astype(bf16).astype(f32)

    weight_wait(2)
    begin = start_of(me)
    own_from = me * width - begin
    valid = lax.broadcasted_iota(jnp.int32, (1, width), 1) >= own_from

    def conv_of(k, s):
        base = pl.multiple_of(s * tokens, 8)
        block = pre[pl.ds(base, tokens + 16), k * width:(k + 1) * width]
        tap = taps_ref[k, :, pl.ds(begin, width)]
        return (tap[0:1] * block[7:7 + tokens] + tap[1:2] * block[8:8 + tokens]
                + tap[2:3] * block[9:9 + tokens])

    def p_copy(s, target, slot):
        return remote(part.at[s, target], got.at[s, slot], p_send.at[s, target], p_recv.at[s, slot],
                      "tp", target)

    for step in range(n):
        s = lax.rem(me + 1 + step, n)
        conv_value, conv_gate = conv_of(0, s), conv_of(1, s)
        hidden = conv_gate * jax.nn.sigmoid(conv_gate) * conv_value
        hidden = jnp.where(valid, hidden, 0.0).astype(bf16)
        per = down.shape[2]
        for k in range(n):
            terms = dot(hidden, down[k]).astype(bf16)
            if per >= cols:
                for j in range(per // cols):
                    part[s, k * (per // cols) + j] = terms[:, j * cols:(j + 1) * cols]
            else:
                ratio = cols // per
                part[s, k // ratio, :, (k % ratio) * per:(k % ratio + 1) * per] = terms
        for offset in range(1, nt):
            p_copy(s, lax.rem(mt + offset, nt), mt).start()

    def s_copy(target, slot):
        return remote(sums.at[target], done.at[slot], s_send.at[target], s_recv.at[slot], "sp", target)

    own = None
    for step in range(n):
        s = lax.rem(me + 1 + step, n)
        total = part[s, mt].astype(f32)
        for offset in range(1, nt):
            peer = lax.rem(mt + offset, nt)
            p_copy(s, peer, mt).wait_send()
            p_copy(s, mt, peer).wait_recv()
            total = total + got[s, peer].astype(f32)
        if step < n - 1:
            sums[s] = total.astype(bf16)
            s_copy(s, me).start()
        else:
            own = total
    for offset in range(1, n):
        peer = lax.rem(me + offset, n)
        s_copy(peer, me).wait_send()
        s_copy(me, peer).wait_recv()
        own = own + done[peer].astype(f32)
    out_ref[...] = (mid[me, mt].astype(f32) + own).astype(bf16)


def packed(wide, narrow):
    def halves(value):
        states = value.shape[3] // 2
        flat = value.reshape(2, -1, 2 * states)
        return flat[..., :states], flat[..., states:]

    wide_parts, narrow_parts = halves(wide), halves(narrow)
    count, states = wide_parts[0].shape[1:]
    small = narrow_parts[0].shape[2]
    top = jnp.concatenate(
        [jnp.pad(part, ((0, 0), (0, 0), (0, LANES - states))) for part in wide_parts], axis=2)
    low = jnp.concatenate(
        [jnp.pad(part, ((0, 0), (0, 0), (states, LANES - states - small))) for part in narrow_parts],
        axis=2)
    return jnp.concatenate([top, low], axis=1)


def on_device(
    n, nt,
    input_wide, input_narrow, spacing, rate_wide, turn_wide, drive_wide, read_wide,
    narrow_decay_rate, turn_narrow, drive_narrow, read_narrow, skip_gain, out_value, out_gate,
    stream, norm_gain, up_value, up_gate, conv_taps, down_weight,
):
    tokens = spacing.shape[0]
    groups = rate_wide.shape[1]
    x = jnp.concatenate([input_wide, input_narrow], axis=1)
    rest = LANES - rate_wide.shape[2] - narrow_decay_rate.shape[2]
    ones = jnp.ones((2, groups, rest), f32)
    rt = jnp.stack([jnp.concatenate([rate_wide, narrow_decay_rate, ones], axis=2),
                    jnp.concatenate([turn_wide, turn_narrow, ones], axis=2)])
    drive = packed(drive_wide, drive_narrow)
    read = packed(read_wide, read_narrow)
    skip = skip_gain.reshape(1, -1)
    extra = -up_value.shape[1] % LANES
    if extra:
        up_value = jnp.pad(up_value, ((0, 0), (0, extra)))
        up_gate = jnp.pad(up_gate, ((0, 0), (0, extra)))
        conv_taps = jnp.pad(conv_taps, ((0, 0), (0, 0), (0, extra)))
        down_weight = jnp.pad(down_weight, ((0, extra), (0, 0)))
    hidden = up_value.shape[1]
    width = -(-hidden // (n * LANES)) * LANES
    rows = up_value.shape[0]
    cols = stream.shape[1]
    per = down_weight.shape[1]
    vmem = pl.BlockSpec(memory_space=pltpu.VMEM)
    anywhere = pl.BlockSpec(memory_space=pl.ANY)
    dma = pltpu.SemaphoreType.DMA
    return pl.pallas_call(
        functools.partial(kernel, n, nt, None),
        out_shape=jax.ShapeDtypeStruct((tokens, cols), bf16),
        in_specs=[pl.BlockSpec(memory_space=pltpu.SMEM)] + [vmem] * 10 + [anywhere] * 3,
        out_specs=vmem,
        scratch_shapes=[
            pltpu.VMEM((rows * n, width), bf16),
            pltpu.VMEM((rows * n, width), bf16),
            pltpu.VMEM((n, width, per), bf16),
            pltpu.VMEM((2, 2, tokens * groups, LANES), f32),
            pltpu.VMEM((2, 2, tokens * groups, LANES), f32),
            pltpu.VMEM((n, 2, 4, groups, LANES), f32),
            pltpu.VMEM((nt, tokens, x.shape[1]), bf16),
            pltpu.VMEM((n, nt, tokens, cols), bf16),
            pltpu.VMEM((nt, 1, cols), f32),
            pltpu.VMEM((n * tokens + 16, 2 * width), f32),
            pltpu.VMEM((n, nt, tokens, cols), bf16),
            pltpu.VMEM((n, nt, tokens, cols), bf16),
            pltpu.VMEM((n, tokens, cols), bf16),
            pltpu.VMEM((n, tokens, cols), bf16),
            dma((3, n)), dma((3, n)), dma((3,)),
            dma((n,)), dma((n,)),
            dma((nt,)), dma((nt,)),
            dma((nt,)), dma((nt,)),
            dma((n,)), dma((n,)),
            dma((n, nt)), dma((n, nt)),
            dma((n, nt)), dma((n, nt)),
            dma((n,)), dma((n,)),
        ],
        compiler_params=pltpu.CompilerParams(
            collective_id=0, has_side_effects=True, vmem_limit_bytes=60 * 1024 * 1024),
    )(spacing, x, rt, drive, read, skip, out_value, out_gate, stream, norm_gain.reshape(1, -1),
      conv_taps, up_value, up_gate, down_weight)


def solution(mesh):
    placed = (
        P(("grp", "sp"), "tp"),
        P(("grp", "sp"), "tp"),
        P(("grp", "sp")),
        P(None, "tp", None),
        P(None, "tp", None),
        P(None, "tp", None, None),
        P(None, "tp", None, None),
        P(None, "tp", None),
        P(None, "tp", None),
        P(None, "tp", None, None),
        P(None, "tp", None, None),
        P(None, "tp"),
        P(None, "tp"),
        P(None, "tp"),
        P(("grp", "sp"), "tp"),
        P("tp"),
        P("sp", "tp"),
        P("sp", "tp"),
        P(None, None, "tp"),
        P("tp", "sp"),
    )
    return jax.shard_map(
        functools.partial(on_device, mesh.shape["sp"], mesh.shape["tp"]),
        mesh=mesh, in_specs=placed, out_specs=P(("grp", "sp"), "tp"), check_vma=False
    )
```

```python
import functools

import jax
import jax.numpy as jnp
from jax import lax
from jax.experimental import pallas as pl
from jax.experimental.pallas import tpu as pltpu
from jax.sharding import PartitionSpec as P

GROUP = 16
LANES = 128
epsilon = 1e-06
f32 = jnp.float32
bf16 = jnp.bfloat16


def sin_cos(angle):
    turns = jnp.round(angle * 0.6366197723675814)
    r = angle - turns * 1.5703125
    r = r - turns * 4.837512969970703125e-4
    r = r - turns * 7.54978995489188216e-8
    z = r * r
    s = ((-1.9515295891e-4 * z + 8.3321608736e-3) * z - 1.6666654611e-1) * z * r + r
    c = ((2.443315711809948e-5 * z - 1.388731625493765e-3) * z + 4.166664568298827e-2) * z * z - 0.5 * z + 1.0
    quadrant = turns.astype(jnp.int32)
    odd = (quadrant & 1) == 1
    sin = jnp.where(odd, c, s)
    cos = jnp.where(odd, s, c)
    sin = jnp.where((quadrant & 2) == 2, -sin, sin)
    cos = jnp.where(((quadrant + 1) & 2) == 2, -cos, cos)
    return sin, cos


def decay_of(rate, turn, span):
    shrink = jnp.exp(-rate * span)
    sin, cos = sin_cos(turn * span)
    return shrink * cos, shrink * sin


def times(ar, ai, br, bi):
    return ar * br - ai * bi, ar * bi + ai * br


def split(value):
    high = value.astype(bf16)
    return high, (value - high.astype(f32)).astype(bf16)


def dot(a, b):
    return jnp.dot(a, b, preferred_element_type=f32)


def dot_nt(a, b):
    return lax.dot_general(a, b, (((1,), (1,)), ((), ())), preferred_element_type=f32)


def kernel(
    n, nt, ng,
    spacing, x_ref, rt_ref, drive_ref, read_ref, skip_ref, ov_ref, og_ref, stream_ref, gain_ref,
    taps_ref, upv_ref, upg_ref, down_ref,
    out_ref,
    upv, upg, down, kick, dec, ends, mix, mid, gain, pre, part, near, got, own, sums, done,
    w_send, w_recv, w_local, y_send, y_recv, e_send, e_recv, g_send, g_recv, m_send, m_recv,
    z_send, z_recv, t_send, f_send, t_recv, d_send, d_recv, p_send, p_recv, s_send, s_recv,
):
    me, mt, mg = lax.axis_index("sp"), lax.axis_index("tp"), lax.axis_index("grp")
    partner = mt + 1 - 2 * lax.rem(mt, 2)
    side = nt // 2
    tokens = x_ref.shape[0]
    groups = rt_ref.shape[2]
    channels = x_ref.shape[1] // 2
    width = upv.shape[1]
    rows = upv_ref.shape[0]
    cols = out_ref.shape[1]
    limit = upv_ref.shape[1] - width

    def remote(src, dst, send, recv, axis, peer):
        return pltpu.make_async_remote_copy(
            src_ref=src, dst_ref=dst, send_sem=send, recv_sem=recv,
            device_id={axis: peer}, device_id_type=pl.DeviceIdType.MESH)

    def start_of(index):
        return pl.multiple_of(jnp.minimum(index * width, limit), LANES)

    barrier = pltpu.get_barrier_semaphore()
    for offset in range(1, n):
        pl.semaphore_signal(barrier, inc=1, device_id={"sp": lax.rem(me + offset, n)},
                            device_id_type=pl.DeviceIdType.MESH)
    for offset in range(1, nt):
        pl.semaphore_signal(barrier, inc=1, device_id={"tp": lax.rem(mt + offset, nt)},
                            device_id_type=pl.DeviceIdType.MESH)
    for offset in range(1, ng):
        pl.semaphore_signal(barrier, inc=1, device_id={"grp": lax.rem(mg + offset, ng)},
                            device_id_type=pl.DeviceIdType.MESH)
    pl.semaphore_wait(barrier, n + nt + ng - 3)

    def weight_parts(which, target, slot, index, count):
        begin = start_of(target)
        full = width if which == 2 else rows
        size = full // count
        first_row = pl.multiple_of(index * size, size)
        if which == 2:
            return (down_ref.at[pl.ds(pl.multiple_of(begin + first_row, GROUP), size), :],
                    down.at[slot, pl.ds(first_row, size), :])
        source, held = ((upv_ref, upv), (upg_ref, upg))[which]
        return (source.at[pl.ds(first_row, size), pl.ds(begin, width)],
                held.at[pl.ds(pl.multiple_of(slot * rows + first_row, size), size), :])

    def weight_copy(which, target, slot):
        src, dst = weight_parts(which, target, slot, mg, ng)
        return remote(src, dst, w_send.at[which, target], w_recv.at[which, slot], "sp", target)

    def share_copy(which, slot, index):
        _, block = weight_parts(which, me, slot, index, ng)
        offset = 1 if index is mg else 0
        return remote(block, block, y_send.at[which, slot], y_recv.at[which, slot], "grp",
                      lax.rem(mg + offset, ng))

    def weight_share(which):
        for offset in range(1, n):
            peer = lax.rem(me + offset, n)
            weight_copy(which, me, peer).wait_recv()
            if ng == 2:
                share_copy(which, peer, mg).start()

    def weight_start(which):
        for offset in range(1, n):
            weight_copy(which, lax.rem(me + offset, n), me).start()

    def weight_wait(which):
        for offset in range(1, n):
            peer = lax.rem(me + offset, n)
            weight_copy(which, peer, me).wait_send()
            if ng == 2:
                share_copy(which, peer, mg).wait_send()
                share_copy(which, peer, 1 - mg).wait_recv()
        src, dst = weight_parts(which, me, me, 0, 1)
        pltpu.make_async_copy(src, dst, w_local.at[which]).wait()

    weight_start(0)
    for which in range(3):
        src, dst = weight_parts(which, me, me, 0, 1)
        pltpu.make_async_copy(src, dst, w_local.at[which]).start()

    def gain_copy(target, slot):
        return remote(gain_ref, gain.at[slot], g_send.at[target], g_recv.at[slot], "tp", target)

    for offset in range(1, nt):
        gain_copy(lax.rem(mt + offset, nt), mt).start()
    gain[mt] = gain_ref[...]

    x = x_ref[...]
    lane_group = lax.rem(lax.broadcasted_iota(jnp.int32, x.shape, 1), channels) // GROUP
    for d in range(2):
        high, low = split(drive_ref[d])
        for g in range(groups):
            picked = jnp.where(lane_group == g, x, jnp.zeros_like(x))
            pushed = dot(picked, high) + dot(picked, low)
            place = pl.ds(g, tokens, stride=groups)
            kick[d, 0, place, :] = pushed[:, :LANES]
            kick[d, 1, place, :] = pushed[:, LANES:]

    rates = [rt_ref[0, d] for d in range(2)]
    turns = [rt_ref[1, d] for d in range(2)]
    inverse = []
    for d in range(2):
        square = rates[d] * rates[d] + turns[d] * turns[d]
        inverse.append((-rates[d] / square, -turns[d] / square))

    def spot(d, i):
        return i if d == 0 else tokens - 1 - i

    def first(i, carry):
        state, total = list(carry[:4]), carry[4]
        for d in range(2):
            t = spot(d, i)
            step = spacing[t]
            if d == 0:
                total = total + step
            place = pl.ds(pl.multiple_of(t * groups, groups), groups)
            dr, di = decay_of(rates[d], turns[d], step)
            cr, ci = times(dr - 1.0, di, *inverse[d])
            kr, ki = times(cr, ci, kick[d, 0, place, :], kick[d, 1, place, :])
            dec[d, 0, place, :] = dr
            dec[d, 1, place, :] = di
            kick[d, 0, place, :] = kr
            kick[d, 1, place, :] = ki
            ar, ai = times(dr, di, state[2 * d], state[2 * d + 1])
            state[2 * d], state[2 * d + 1] = ar + kr, ai + ki
        return (*state, total)

    zero = jnp.zeros((groups, LANES), f32)
    found = lax.fori_loop(0, tokens, first, (zero, zero, zero, zero, jnp.float32(0.0)), unroll=4)
    for d in range(2):
        ar, ai = decay_of(rates[d], turns[d], found[4])
        ends[me, d, 0] = found[2 * d]
        ends[me, d, 1] = found[2 * d + 1]
        ends[me, d, 2] = ar
        ends[me, d, 3] = ai

    def ends_copy(target, slot):
        return remote(ends.at[slot], ends.at[slot], e_send.at[target], e_recv.at[slot], "sp", target)

    for offset in range(1, n):
        ends_copy(lax.rem(me + offset, n), me).start()
    weight_start(1)
    for offset in range(1, n):
        peer = lax.rem(me + offset, n)
        ends_copy(peer, me).wait_send()
        ends_copy(me, peer).wait_recv()

    carry = []
    for d in range(2):
        cr, ci = zero, zero
        for k in range(n):
            s = k if d == 0 else n - 1 - k
            use = (s < me) if d == 0 else (s > me)
            nr, ni = times(ends[s, d, 2], ends[s, d, 3], cr, ci)
            flag = jnp.where(use, 1, 0)
            keep = jnp.full((groups, LANES), flag, jnp.int32) == 1
            cr = jnp.where(keep, nr + ends[s, d, 0], cr)
            ci = jnp.where(keep, ni + ends[s, d, 1], ci)
        carry += [cr, ci]
    weight_share(0)

    def second(i, carry):
        state = list(carry)
        for d in range(2):
            t = spot(d, i)
            place = pl.ds(pl.multiple_of(t * groups, groups), groups)
            ar, ai = times(dec[d, 0, place, :], dec[d, 1, place, :], state[2 * d], state[2 * d + 1])
            state[2 * d] = ar + kick[d, 0, place, :]
            state[2 * d + 1] = ai + kick[d, 1, place, :]
            kick[d, 0, place, :] = state[2 * d]
            kick[d, 1, place, :] = state[2 * d + 1]
        return tuple(state)

    lax.fori_loop(0, tokens, second, tuple(carry), unroll=4)

    reading = skip_ref[...] * x.astype(f32)
    for d in range(2):
        high, low = split(read_ref[d])
        for g in range(groups):
            place = pl.ds(g, tokens, stride=groups)
            state = jnp.concatenate([kick[d, 0, place, :], kick[d, 1, place, :]], axis=1)
            state_high, state_low = split(state)
            value = dot_nt(state_high, high) + dot_nt(state_low, high) + dot_nt(state_high, low)
            reading = reading + jnp.where(lane_group == g, value, 0.0)
    mix[mt] = jax.nn.gelu(reading).astype(bf16)

    def mix_copy(target, slot):
        return remote(mix.at[slot], mix.at[slot], m_send.at[target], m_recv.at[slot], "tp", target)

    for offset in range(1, nt):
        mix_copy(lax.rem(mt + offset, nt), mt).start()
    for offset in range(1, nt):
        peer = lax.rem(mt + offset, nt)
        mix_copy(peer, mt).wait_send()
        mix_copy(mt, peer).wait_recv()

    weight_share(1)
    value = jnp.zeros((tokens, cols), f32)
    gate = jnp.zeros((tokens, cols), f32)
    half = ov_ref.shape[0] // 2
    for k in range(nt):
        for h in range(2):
            piece = mix[k][:, h * channels:(h + 1) * channels]
            at = slice(h * half + k * channels, h * half + (k + 1) * channels)
            value = value + dot(piece, ov_ref[at, :])
            gate = gate + dot(piece, og_ref[at, :])
    mid[me, mt] = (stream_ref[...].astype(f32) + value * jax.nn.sigmoid(gate)).astype(bf16)

    def z_copy(target, slot):
        return remote(mid.at[slot, mt], mid.at[slot, mt], z_send.at[target], z_recv.at[slot], "sp", target)

    def t_copy(s, target, slot):
        return remote(mid.at[s, slot], mid.at[s, slot], t_send.at[s, target], t_recv.at[s, slot], "tp", target)

    def f_copy(s, slot):
        return remote(mid.at[s, slot], mid.at[s, slot], f_send.at[s, slot], t_recv.at[s, slot], "tp", partner)

    def spread(s):
        for offset in range(1, side):
            t_copy(s, lax.rem(mt + 2 * offset, nt), mt).start()
        f_copy(s, mt).start()

    def relay(s):
        for offset in range(1, side):
            peer = lax.rem(mt + 2 * offset, nt)
            t_copy(s, mt, peer).wait_recv()
            f_copy(s, peer).start()

    for offset in range(1, n):
        z_copy(lax.rem(me + offset, n), me).start()
    spread(me)
    weight_start(2)
    for offset in range(1, n):
        peer = lax.rem(me + offset, n)
        z_copy(me, peer).wait_recv()
        spread(peer)
        relay(lax.rem(me + offset - 1, n))
    relay(lax.rem(me + n - 1, n))
    for offset in range(1, nt):
        peer = lax.rem(mt + offset, nt)
        gain_copy(peer, mt).wait_send()
        gain_copy(mt, peer).wait_recv()
    weight_wait(0)
    weight_wait(1)
    for offset in range(1, n):
        z_copy(lax.rem(me + offset, n), me).wait_send()
    weight_share(2)

    for i in range(2):
        pre[pl.ds(i * (8 + n * tokens), 8), :] = jnp.zeros((8, 2 * width), f32)
    for step in range(n):
        s = lax.rem(me + step, n)
        for offset in range(side):
            peer = lax.rem(mt + 2 * offset, nt)
            if offset:
                t_copy(s, peer, mt).wait_send()
            f_copy(s, peer).wait_send()
            f_copy(s, lax.rem(partner + 2 * offset, nt)).wait_recv()
        squares = jnp.zeros((tokens, 1), f32)
        for k in range(nt):
            piece = mid[s, k].astype(f32)
            squares = squares + jnp.sum(piece * piece, axis=1, keepdims=True)
        scale = lax.rsqrt(squares / (nt * cols) + epsilon)
        normed = jnp.concatenate(
            [(mid[s, k].astype(f32) * scale * gain[k]).astype(bf16) for k in range(nt)], axis=1)
        place = pl.ds(pl.multiple_of(8 + s * tokens, 8), tokens)
        pre[place, :width] = dot(normed, upv[...]).astype(bf16).astype(f32)
        pre[place, width:] = dot(normed, upg[...]).astype(bf16).astype(f32)

    weight_wait(2)
    begin = start_of(me)
    own_from = me * width - begin
    valid = lax.broadcasted_iota(jnp.int32, (1, width), 1) >= own_from

    def conv_of(k, s):
        base = pl.multiple_of(s * tokens, 8)
        block = pre[pl.ds(base, tokens + 16), k * width:(k + 1) * width]
        tap = taps_ref[k, :, pl.ds(begin, width)]
        return (tap[0:1] * block[7:7 + tokens] + tap[1:2] * block[8:8 + tokens]
                + tap[2:3] * block[9:9 + tokens])

    def d_copy(s, target):
        return remote(part.at[s, target], near.at[s, target], d_send.at[s, target], d_recv.at[s, target],
                      "tp", partner)

    def p_copy(s, target, slot):
        return remote(part.at[s, target], got.at[s, slot], p_send.at[s, target], p_recv.at[s, slot],
                      "tp", target)

    def pass_on(s):
        for offset in range(side):
            target = lax.rem(mt + 2 * offset, nt)
            d_copy(s, target).wait_recv()
            total = part[s, target].astype(f32) + near[s, target].astype(f32)
            if offset:
                part[s, target] = total.astype(bf16)
                p_copy(s, target, mt).start()
            else:
                own[s] = total

    for step in range(n):
        s = lax.rem(me + 1 + step, n)
        conv_value, conv_gate = conv_of(0, s), conv_of(1, s)
        hidden = conv_gate * jax.nn.sigmoid(conv_gate) * conv_value
        hidden = jnp.where(valid, hidden, 0.0).astype(bf16)
        per = down.shape[2]
        for k in range(n):
            terms = dot(hidden, down[k]).astype(bf16)
            if per >= cols:
                for j in range(per // cols):
                    part[s, k * (per // cols) + j] = terms[:, j * cols:(j + 1) * cols]
            else:
                ratio = cols // per
                part[s, k // ratio, :, (k % ratio) * per:(k % ratio + 1) * per] = terms
        for offset in range(side):
            d_copy(s, lax.rem(partner + 2 * offset, nt)).start()
        if step:
            pass_on(lax.rem(me + step, n))
    pass_on(me)

    def s_copy(target, slot):
        return remote(sums.at[target], done.at[slot], s_send.at[target], s_recv.at[slot], "sp", target)

    for step in range(n):
        s = lax.rem(me + 1 + step, n)
        total = own[s]
        for offset in range(side):
            d_copy(s, lax.rem(partner + 2 * offset, nt)).wait_send()
            if offset:
                peer = lax.rem(mt + 2 * offset, nt)
                p_copy(s, peer, mt).wait_send()
                p_copy(s, mt, peer).wait_recv()
                total = total + got[s, peer].astype(f32)
        if step < n - 1:
            sums[s] = total.astype(bf16)
            s_copy(s, me).start()
    for offset in range(1, n):
        peer = lax.rem(me + offset, n)
        s_copy(peer, me).wait_send()
        s_copy(me, peer).wait_recv()
        total = total + done[peer].astype(f32)
    out_ref[...] = (mid[me, mt].astype(f32) + total).astype(bf16)


def packed(wide, narrow):
    def halves(value):
        states = value.shape[3] // 2
        flat = value.reshape(2, -1, 2 * states)
        return flat[..., :states], flat[..., states:]

    wide_parts, narrow_parts = halves(wide), halves(narrow)
    count, states = wide_parts[0].shape[1:]
    small = narrow_parts[0].shape[2]
    top = jnp.concatenate(
        [jnp.pad(part, ((0, 0), (0, 0), (0, LANES - states))) for part in wide_parts], axis=2)
    low = jnp.concatenate(
        [jnp.pad(part, ((0, 0), (0, 0), (states, LANES - states - small))) for part in narrow_parts],
        axis=2)
    return jnp.concatenate([top, low], axis=1)


def on_device(
    n, nt, ng,
    input_wide, input_narrow, spacing, rate_wide, turn_wide, drive_wide, read_wide,
    narrow_decay_rate, turn_narrow, drive_narrow, read_narrow, skip_gain, out_value, out_gate,
    stream, norm_gain, up_value, up_gate, conv_taps, down_weight,
):
    tokens = spacing.shape[0]
    groups = rate_wide.shape[1]
    x = jnp.concatenate([input_wide, input_narrow], axis=1)
    rest = LANES - rate_wide.shape[2] - narrow_decay_rate.shape[2]
    ones = jnp.ones((2, groups, rest), f32)
    rt = jnp.stack([jnp.concatenate([rate_wide, narrow_decay_rate, ones], axis=2),
                    jnp.concatenate([turn_wide, turn_narrow, ones], axis=2)])
    drive = packed(drive_wide, drive_narrow)
    read = packed(read_wide, read_narrow)
    skip = skip_gain.reshape(1, -1)
    extra = -up_value.shape[1] % LANES
    if extra:
        up_value = jnp.pad(up_value, ((0, 0), (0, extra)))
        up_gate = jnp.pad(up_gate, ((0, 0), (0, extra)))
        conv_taps = jnp.pad(conv_taps, ((0, 0), (0, 0), (0, extra)))
        down_weight = jnp.pad(down_weight, ((0, extra), (0, 0)))
    hidden = up_value.shape[1]
    width = -(-hidden // (n * LANES)) * LANES
    rows = up_value.shape[0]
    cols = stream.shape[1]
    per = down_weight.shape[1]
    vmem = pl.BlockSpec(memory_space=pltpu.VMEM)
    anywhere = pl.BlockSpec(memory_space=pl.ANY)
    dma = pltpu.SemaphoreType.DMA
    return pl.pallas_call(
        functools.partial(kernel, n, nt, ng),
        out_shape=jax.ShapeDtypeStruct((tokens, cols), bf16),
        in_specs=[pl.BlockSpec(memory_space=pltpu.SMEM)] + [vmem] * 10 + [anywhere] * 3,
        out_specs=vmem,
        scratch_shapes=[
            pltpu.VMEM((rows * n, width), bf16),
            pltpu.VMEM((rows * n, width), bf16),
            pltpu.VMEM((n, width, per), bf16),
            pltpu.VMEM((2, 2, tokens * groups, LANES), f32),
            pltpu.VMEM((2, 2, tokens * groups, LANES), f32),
            pltpu.VMEM((n, 2, 4, groups, LANES), f32),
            pltpu.VMEM((nt, tokens, x.shape[1]), bf16),
            pltpu.VMEM((n, nt, tokens, cols), bf16),
            pltpu.VMEM((nt, 1, cols), f32),
            pltpu.VMEM((n * tokens + 16, 2 * width), f32),
            pltpu.VMEM((n, nt, tokens, cols), bf16),
            pltpu.VMEM((n, nt, tokens, cols), bf16),
            pltpu.VMEM((n, nt, tokens, cols), bf16),
            pltpu.VMEM((n, tokens, cols), f32),
            pltpu.VMEM((n, tokens, cols), bf16),
            pltpu.VMEM((n, tokens, cols), bf16),
            dma((3, n)), dma((3, n)), dma((3,)), dma((3, n)), dma((3, n)),
            dma((n,)), dma((n,)),
            dma((nt,)), dma((nt,)),
            dma((nt,)), dma((nt,)),
            dma((n,)), dma((n,)),
            dma((n, nt)), dma((n, nt)), dma((n, nt)),
            dma((n, nt)), dma((n, nt)),
            dma((n, nt)), dma((n, nt)),
            dma((n,)), dma((n,)),
        ],
        compiler_params=pltpu.CompilerParams(
            collective_id=0, has_side_effects=True, vmem_limit_bytes=60 * 1024 * 1024),
    )(spacing, x, rt, drive, read, skip, out_value, out_gate, stream, norm_gain.reshape(1, -1),
      conv_taps, up_value, up_gate, down_weight)


def solution(mesh):
    placed = (
        P(("grp", "sp"), "tp"),
        P(("grp", "sp"), "tp"),
        P(("grp", "sp")),
        P(None, "tp", None),
        P(None, "tp", None),
        P(None, "tp", None, None),
        P(None, "tp", None, None),
        P(None, "tp", None),
        P(None, "tp", None),
        P(None, "tp", None, None),
        P(None, "tp", None, None),
        P(None, "tp"),
        P(None, "tp"),
        P(None, "tp"),
        P(("grp", "sp"), "tp"),
        P("tp"),
        P("sp", "tp"),
        P("sp", "tp"),
        P(None, None, "tp"),
        P("tp", "sp"),
    )
    return jax.shard_map(
        functools.partial(on_device, mesh.shape["sp"], mesh.shape["tp"], mesh.shape["grp"]),
        mesh=mesh, in_specs=placed, out_specs=P(("grp", "sp"), "tp"), check_vma=False
    )
```

```python
import functools

import jax
import jax.numpy as jnp
from jax import lax
from jax.experimental import pallas as pl
from jax.experimental.pallas import tpu as pltpu
from jax.sharding import PartitionSpec as P

GROUP = 16
LANES = 128
epsilon = 1e-06
f32 = jnp.float32
bf16 = jnp.bfloat16


def sin_cos(angle):
    turns = jnp.round(angle * 0.6366197723675814)
    r = angle - turns * 1.5703125
    r = r - turns * 4.837512969970703125e-4
    r = r - turns * 7.54978995489188216e-8
    z = r * r
    s = ((-1.9515295891e-4 * z + 8.3321608736e-3) * z - 1.6666654611e-1) * z * r + r
    c = ((2.443315711809948e-5 * z - 1.388731625493765e-3) * z + 4.166664568298827e-2) * z * z - 0.5 * z + 1.0
    quadrant = turns.astype(jnp.int32)
    odd = (quadrant & 1) == 1
    sin = jnp.where(odd, c, s)
    cos = jnp.where(odd, s, c)
    sin = jnp.where((quadrant & 2) == 2, -sin, sin)
    cos = jnp.where(((quadrant + 1) & 2) == 2, -cos, cos)
    return sin, cos


def decay_of(rate, turn, span):
    shrink = jnp.exp(-rate * span)
    sin, cos = sin_cos(turn * span)
    return shrink * cos, shrink * sin


def times(ar, ai, br, bi):
    return ar * br - ai * bi, ar * bi + ai * br


def split(value):
    high = value.astype(bf16)
    return high, (value - high.astype(f32)).astype(bf16)


def dot(a, b):
    return jnp.dot(a, b, preferred_element_type=f32)


def dot_nt(a, b):
    return lax.dot_general(a, b, (((1,), (1,)), ((), ())), preferred_element_type=f32)


def packed(wide, narrow):
    wide = wide.reshape(-1, wide.shape[-1])
    narrow = narrow.reshape(-1, narrow.shape[-1])
    states, small = wide.shape[1] // 2, narrow.shape[1] // 2

    def zeros(like, lanes):
        return jnp.zeros((like.shape[0], lanes), f32)

    top = jnp.concatenate(
        [wide[:, :states], zeros(wide, LANES - states), wide[:, states:], zeros(wide, LANES - states)], axis=1)
    low = jnp.concatenate(
        [zeros(narrow, states), narrow[:, :small], zeros(narrow, LANES - small),
         narrow[:, small:], zeros(narrow, LANES - states - small)], axis=1)
    return jnp.concatenate([top, low], axis=0)


def kernel(
    n, nt, ng,
    spacing, xw_ref, xn_ref, rw_ref, tw_ref, rn_ref, tn_ref, dw_ref, dn_ref, rdw_ref, rdn_ref, skip_ref, ov_ref, og_ref, stream_ref, gain_ref,
    taps_ref, upv_ref, upg_ref, down_ref,
    out_ref,
    upv, upg, down, kick, dec, ends, mix, mid, gain, pre, part, near, got, own, sums, done,
    w_send, w_recv, w_local, y_send, y_recv, e_send, e_recv, g_send, g_recv, m_send, m_recv,
    z_send, z_recv, t_send, f_send, t_recv, d_send, d_recv, p_send, p_recv, s_send, s_recv,
):
    me, mt, mg = lax.axis_index("sp"), lax.axis_index("tp"), lax.axis_index("grp")
    partner = mt + 1 - 2 * lax.rem(mt, 2)
    side = nt // 2
    tokens, channels = xw_ref.shape
    groups = rw_ref.shape[1]
    width = upv.shape[1]
    rows = upv_ref.shape[0]
    cols = out_ref.shape[1]
    limit = upv_ref.shape[1] - width

    def remote(src, dst, send, recv, axis, peer):
        return pltpu.make_async_remote_copy(
            src_ref=src, dst_ref=dst, send_sem=send, recv_sem=recv,
            device_id={axis: peer}, device_id_type=pl.DeviceIdType.MESH)

    def start_of(index):
        return pl.multiple_of(jnp.minimum(index * width, limit), LANES)

    barrier = pltpu.get_barrier_semaphore()
    for offset in range(1, n):
        pl.semaphore_signal(barrier, inc=1, device_id={"sp": lax.rem(me + offset, n)},
                            device_id_type=pl.DeviceIdType.MESH)
    for offset in range(1, nt):
        pl.semaphore_signal(barrier, inc=1, device_id={"tp": lax.rem(mt + offset, nt)},
                            device_id_type=pl.DeviceIdType.MESH)
    for offset in range(1, ng):
        pl.semaphore_signal(barrier, inc=1, device_id={"grp": lax.rem(mg + offset, ng)},
                            device_id_type=pl.DeviceIdType.MESH)
    pl.semaphore_wait(barrier, n + nt + ng - 3)

    def weight_parts(which, target, slot, index, count):
        begin = start_of(target)
        full = width if which == 2 else rows
        size = full // count
        first_row = pl.multiple_of(index * size, size)
        if which == 2:
            return (down_ref.at[pl.ds(pl.multiple_of(begin + first_row, GROUP), size), :],
                    down.at[slot, pl.ds(first_row, size), :])
        source, held = ((upv_ref, upv), (upg_ref, upg))[which]
        return (source.at[pl.ds(first_row, size), pl.ds(begin, width)],
                held.at[pl.ds(pl.multiple_of(slot * rows + first_row, size), size), :])

    def weight_copy(which, target, slot):
        src, dst = weight_parts(which, target, slot, mg, ng)
        return remote(src, dst, w_send.at[which, target], w_recv.at[which, slot], "sp", target)

    def share_copy(which, slot, index):
        _, block = weight_parts(which, me, slot, index, ng)
        offset = 1 if index is mg else 0
        return remote(block, block, y_send.at[which, slot], y_recv.at[which, slot], "grp",
                      lax.rem(mg + offset, ng))

    def weight_share(which):
        for offset in range(1, n):
            peer = lax.rem(me + offset, n)
            weight_copy(which, me, peer).wait_recv()
            if ng == 2:
                share_copy(which, peer, mg).start()

    def weight_start(which):
        for offset in range(1, n):
            weight_copy(which, lax.rem(me + offset, n), me).start()

    def weight_wait(which):
        for offset in range(1, n):
            peer = lax.rem(me + offset, n)
            weight_copy(which, peer, me).wait_send()
            if ng == 2:
                share_copy(which, peer, mg).wait_send()
                share_copy(which, peer, 1 - mg).wait_recv()
        src, dst = weight_parts(which, me, me, 0, 1)
        pltpu.make_async_copy(src, dst, w_local.at[which]).wait()

    weight_start(0)
    for which in range(3):
        src, dst = weight_parts(which, me, me, 0, 1)
        pltpu.make_async_copy(src, dst, w_local.at[which]).start()

    def gain_copy(target, slot):
        return remote(gain_ref, gain.at[slot], g_send.at[target], g_recv.at[slot], "tp", target)

    for offset in range(1, nt):
        gain_copy(lax.rem(mt + offset, nt), mt).start()
    gain[mt] = gain_ref[...]

    x = jnp.concatenate([xw_ref[...], xn_ref[...]], axis=1)
    rest = jnp.ones((groups, LANES - rw_ref.shape[2] - rn_ref.shape[2]), f32)
    lane_group = lax.rem(lax.broadcasted_iota(jnp.int32, x.shape, 1), channels) // GROUP
    for d in range(2):
        high, low = split(packed(dw_ref[d], dn_ref[d]))
        for g in range(groups):
            picked = jnp.where(lane_group == g, x, jnp.zeros_like(x))
            pushed = dot(picked, high) + dot(picked, low)
            place = pl.ds(g, tokens, stride=groups)
            kick[d, 0, place, :] = pushed[:, :LANES]
            kick[d, 1, place, :] = pushed[:, LANES:]

    rates = [jnp.concatenate([rw_ref[d], rn_ref[d], rest], axis=1) for d in range(2)]
    turns = [jnp.concatenate([tw_ref[d], tn_ref[d], rest], axis=1) for d in range(2)]
    inverse = []
    for d in range(2):
        square = rates[d] * rates[d] + turns[d] * turns[d]
        inverse.append((-rates[d] / square, -turns[d] / square))

    def spot(d, i):
        return i if d == 0 else tokens - 1 - i

    def first(i, carry):
        state, total = list(carry[:4]), carry[4]
        for d in range(2):
            t = spot(d, i)
            step = spacing[t]
            if d == 0:
                total = total + step
            place = pl.ds(pl.multiple_of(t * groups, groups), groups)
            dr, di = decay_of(rates[d], turns[d], step)
            cr, ci = times(dr - 1.0, di, *inverse[d])
            kr, ki = times(cr, ci, kick[d, 0, place, :], kick[d, 1, place, :])
            dec[d, 0, place, :] = dr
            dec[d, 1, place, :] = di
            kick[d, 0, place, :] = kr
            kick[d, 1, place, :] = ki
            ar, ai = times(dr, di, state[2 * d], state[2 * d + 1])
            state[2 * d], state[2 * d + 1] = ar + kr, ai + ki
        return (*state, total)

    zero = jnp.zeros((groups, LANES), f32)
    found = lax.fori_loop(0, tokens, first, (zero, zero, zero, zero, jnp.float32(0.0)), unroll=4)
    for d in range(2):
        ar, ai = decay_of(rates[d], turns[d], found[4])
        ends[me, d, 0] = found[2 * d]
        ends[me, d, 1] = found[2 * d + 1]
        ends[me, d, 2] = ar
        ends[me, d, 3] = ai

    def ends_copy(target, slot):
        return remote(ends.at[slot], ends.at[slot], e_send.at[target], e_recv.at[slot], "sp", target)

    for offset in range(1, n):
        ends_copy(lax.rem(me + offset, n), me).start()
    weight_start(1)
    weight_start(2)
    for offset in range(1, n):
        peer = lax.rem(me + offset, n)
        ends_copy(peer, me).wait_send()
        ends_copy(me, peer).wait_recv()

    carry = []
    for d in range(2):
        cr, ci = zero, zero
        for k in range(n):
            s = k if d == 0 else n - 1 - k
            use = (s < me) if d == 0 else (s > me)
            nr, ni = times(ends[s, d, 2], ends[s, d, 3], cr, ci)
            flag = jnp.where(use, 1, 0)
            keep = jnp.full((groups, LANES), flag, jnp.int32) == 1
            cr = jnp.where(keep, nr + ends[s, d, 0], cr)
            ci = jnp.where(keep, ni + ends[s, d, 1], ci)
        carry += [cr, ci]
    weight_share(0)

    def second(i, carry):
        state = list(carry)
        for d in range(2):
            t = spot(d, i)
            place = pl.ds(pl.multiple_of(t * groups, groups), groups)
            ar, ai = times(dec[d, 0, place, :], dec[d, 1, place, :], state[2 * d], state[2 * d + 1])
            state[2 * d] = ar + kick[d, 0, place, :]
            state[2 * d + 1] = ai + kick[d, 1, place, :]
            kick[d, 0, place, :] = state[2 * d]
            kick[d, 1, place, :] = state[2 * d + 1]
        return tuple(state)

    lax.fori_loop(0, tokens, second, tuple(carry), unroll=4)

    reading = jnp.concatenate([skip_ref[0:1, :], skip_ref[1:2, :]], axis=1) * x.astype(f32)
    for d in range(2):
        high, low = split(packed(rdw_ref[d], rdn_ref[d]))
        for g in range(groups):
            place = pl.ds(g, tokens, stride=groups)
            state = jnp.concatenate([kick[d, 0, place, :], kick[d, 1, place, :]], axis=1)
            state_high, state_low = split(state)
            value = dot_nt(state_high, high) + dot_nt(state_low, high) + dot_nt(state_high, low)
            reading = reading + jnp.where(lane_group == g, value, 0.0)
    mix[mt] = jax.nn.gelu(reading).astype(bf16)

    def mix_copy(target, slot):
        return remote(mix.at[slot], mix.at[slot], m_send.at[target], m_recv.at[slot], "tp", target)

    for offset in range(1, nt):
        mix_copy(lax.rem(mt + offset, nt), mt).start()
    for offset in range(1, nt):
        peer = lax.rem(mt + offset, nt)
        mix_copy(peer, mt).wait_send()
        mix_copy(mt, peer).wait_recv()

    weight_share(1)
    value = jnp.zeros((tokens, cols), f32)
    gate = jnp.zeros((tokens, cols), f32)
    half = ov_ref.shape[0] // 2
    for k in range(nt):
        for h in range(2):
            piece = mix[k][:, h * channels:(h + 1) * channels]
            at = slice(h * half + k * channels, h * half + (k + 1) * channels)
            value = value + dot(piece, ov_ref[at, :])
            gate = gate + dot(piece, og_ref[at, :])
    mid[me, mt] = (stream_ref[...].astype(f32) + value * jax.nn.sigmoid(gate)).astype(bf16)

    def z_copy(target, slot):
        return remote(mid.at[slot, mt], mid.at[slot, mt], z_send.at[target], z_recv.at[slot], "sp", target)

    def t_copy(s, target, slot):
        return remote(mid.at[s, slot], mid.at[s, slot], t_send.at[s, target], t_recv.at[s, slot], "tp", target)

    def f_copy(s, slot):
        return remote(mid.at[s, slot], mid.at[s, slot], f_send.at[s, slot], t_recv.at[s, slot], "tp", partner)

    def spread(s):
        for offset in range(1, side):
            t_copy(s, lax.rem(mt + 2 * offset, nt), mt).start()
        f_copy(s, mt).start()

    def relay(s):
        for offset in range(1, side):
            peer = lax.rem(mt + 2 * offset, nt)
            t_copy(s, mt, peer).wait_recv()
            f_copy(s, peer).start()

    for offset in range(1, n):
        z_copy(lax.rem(me + offset, n), me).start()
    spread(me)
    for offset in range(1, nt):
        peer = lax.rem(mt + offset, nt)
        gain_copy(peer, mt).wait_send()
        gain_copy(mt, peer).wait_recv()
    for i in range(2):
        pre[pl.ds(i * (8 + n * tokens), 8), :] = jnp.zeros((8, 2 * width), f32)
    weight_share(2)
    relay(me)
    weight_wait(0)
    weight_wait(1)

    def raise_block(s):
        for offset in range(side):
            peer = lax.rem(mt + 2 * offset, nt)
            if offset:
                t_copy(s, peer, mt).wait_send()
            f_copy(s, peer).wait_send()
            f_copy(s, lax.rem(partner + 2 * offset, nt)).wait_recv()
        squares = jnp.zeros((tokens, 1), f32)
        for k in range(nt):
            piece = mid[s, k].astype(f32)
            squares = squares + jnp.sum(piece * piece, axis=1, keepdims=True)
        scale = lax.rsqrt(squares / (nt * cols) + epsilon)
        normed = jnp.concatenate(
            [(mid[s, k].astype(f32) * scale * gain[k]).astype(bf16) for k in range(nt)], axis=1)
        place = pl.ds(pl.multiple_of(8 + s * tokens, 8), tokens)
        pre[place, :width] = dot(normed, upv[...]).astype(bf16).astype(f32)
        pre[place, width:] = dot(normed, upg[...]).astype(bf16).astype(f32)

    for offset in range(1, n):
        peer = lax.rem(me + offset, n)
        z_copy(me, peer).wait_recv()
        spread(peer)
        raise_block(lax.rem(me + offset - 1, n))
        relay(peer)
    raise_block(lax.rem(me + n - 1, n))
    for offset in range(1, n):
        z_copy(lax.rem(me + offset, n), me).wait_send()

    weight_wait(2)
    begin = start_of(me)
    own_from = me * width - begin
    valid = lax.broadcasted_iota(jnp.int32, (1, width), 1) >= own_from

    def conv_of(k, s):
        base = pl.multiple_of(s * tokens, 8)
        block = pre[pl.ds(base, tokens + 16), k * width:(k + 1) * width]
        tap = taps_ref[k, :, pl.ds(begin, width)]
        return (tap[0:1] * block[7:7 + tokens] + tap[1:2] * block[8:8 + tokens]
                + tap[2:3] * block[9:9 + tokens])

    def d_copy(s, target):
        return remote(part.at[s, target], near.at[s, target], d_send.at[s, target], d_recv.at[s, target],
                      "tp", partner)

    def p_copy(s, target, slot):
        return remote(part.at[s, target], got.at[s, slot], p_send.at[s, target], p_recv.at[s, slot],
                      "tp", target)

    def pass_on(s):
        for offset in range(side):
            target = lax.rem(mt + 2 * offset, nt)
            d_copy(s, target).wait_recv()
            total = part[s, target].astype(f32) + near[s, target].astype(f32)
            if offset:
                part[s, target] = total.astype(bf16)
                p_copy(s, target, mt).start()
            else:
                own[s] = total

    for step in range(n):
        s = lax.rem(me + 1 + step, n)
        conv_value, conv_gate = conv_of(0, s), conv_of(1, s)
        hidden = conv_gate * jax.nn.sigmoid(conv_gate) * conv_value
        hidden = jnp.where(valid, hidden, 0.0).astype(bf16)
        per = down.shape[2]
        for k in range(n):
            terms = dot(hidden, down[k]).astype(bf16)
            if per >= cols:
                for j in range(per // cols):
                    part[s, k * (per // cols) + j] = terms[:, j * cols:(j + 1) * cols]
            else:
                ratio = cols // per
                part[s, k // ratio, :, (k % ratio) * per:(k % ratio + 1) * per] = terms
        for offset in range(side):
            d_copy(s, lax.rem(partner + 2 * offset, nt)).start()
        if step:
            pass_on(lax.rem(me + step, n))
    pass_on(me)

    def s_copy(target, slot):
        return remote(sums.at[target], done.at[slot], s_send.at[target], s_recv.at[slot], "sp", target)

    for step in range(n):
        s = lax.rem(me + 1 + step, n)
        total = own[s]
        for offset in range(side):
            d_copy(s, lax.rem(partner + 2 * offset, nt)).wait_send()
            if offset:
                peer = lax.rem(mt + 2 * offset, nt)
                p_copy(s, peer, mt).wait_send()
                p_copy(s, mt, peer).wait_recv()
                total = total + got[s, peer].astype(f32)
        if step < n - 1:
            sums[s] = total.astype(bf16)
            s_copy(s, me).start()
    for offset in range(1, n):
        peer = lax.rem(me + offset, n)
        s_copy(peer, me).wait_send()
        s_copy(me, peer).wait_recv()
        total = total + done[peer].astype(f32)
    out_ref[...] = (mid[me, mt].astype(f32) + total).astype(bf16)


def on_device(
    n, nt, ng,
    input_wide, input_narrow, spacing, rate_wide, turn_wide, drive_wide, read_wide,
    narrow_decay_rate, turn_narrow, drive_narrow, read_narrow, skip_gain, out_value, out_gate,
    stream, norm_gain, up_value, up_gate, conv_taps, down_weight,
):
    tokens = spacing.shape[0]
    groups = rate_wide.shape[1]
    extra = -up_value.shape[1] % LANES
    if extra:
        up_value = jnp.pad(up_value, ((0, 0), (0, extra)))
        up_gate = jnp.pad(up_gate, ((0, 0), (0, extra)))
        conv_taps = jnp.pad(conv_taps, ((0, 0), (0, 0), (0, extra)))
        down_weight = jnp.pad(down_weight, ((0, extra), (0, 0)))
    hidden = up_value.shape[1]
    width = -(-hidden // (n * LANES)) * LANES
    rows = up_value.shape[0]
    cols = stream.shape[1]
    per = down_weight.shape[1]
    vmem = pl.BlockSpec(memory_space=pltpu.VMEM)
    anywhere = pl.BlockSpec(memory_space=pl.ANY)
    dma = pltpu.SemaphoreType.DMA
    return pl.pallas_call(
        functools.partial(kernel, n, nt, ng),
        out_shape=jax.ShapeDtypeStruct((tokens, cols), bf16),
        in_specs=[pl.BlockSpec(memory_space=pltpu.SMEM)] + [vmem] * 16 + [anywhere] * 3,
        out_specs=vmem,
        scratch_shapes=[
            pltpu.VMEM((rows * n, width), bf16),
            pltpu.VMEM((rows * n, width), bf16),
            pltpu.VMEM((n, width, per), bf16),
            pltpu.VMEM((2, 2, tokens * groups, LANES), f32),
            pltpu.VMEM((2, 2, tokens * groups, LANES), f32),
            pltpu.VMEM((n, 2, 4, groups, LANES), f32),
            pltpu.VMEM((nt, tokens, 2 * input_wide.shape[1]), bf16),
            pltpu.VMEM((n, nt, tokens, cols), bf16),
            pltpu.VMEM((nt, 1, cols), f32),
            pltpu.VMEM((n * tokens + 16, 2 * width), f32),
            pltpu.VMEM((n, nt, tokens, cols), bf16),
            pltpu.VMEM((n, nt, tokens, cols), bf16),
            pltpu.VMEM((n, nt, tokens, cols), bf16),
            pltpu.VMEM((n, tokens, cols), f32),
            pltpu.VMEM((n, tokens, cols), bf16),
            pltpu.VMEM((n, tokens, cols), bf16),
            dma((3, n)), dma((3, n)), dma((3,)), dma((3, n)), dma((3, n)),
            dma((n,)), dma((n,)),
            dma((nt,)), dma((nt,)),
            dma((nt,)), dma((nt,)),
            dma((n,)), dma((n,)),
            dma((n, nt)), dma((n, nt)), dma((n, nt)),
            dma((n, nt)), dma((n, nt)),
            dma((n, nt)), dma((n, nt)),
            dma((n,)), dma((n,)),
        ],
        compiler_params=pltpu.CompilerParams(
            collective_id=0, has_side_effects=True, vmem_limit_bytes=60 * 1024 * 1024),
    )(spacing, input_wide, input_narrow, rate_wide, turn_wide, narrow_decay_rate, turn_narrow,
      drive_wide, drive_narrow, read_wide, read_narrow, skip_gain, out_value, out_gate, stream, norm_gain.reshape(1, -1),
      conv_taps, up_value, up_gate, down_weight)


def solution(mesh):
    placed = (
        P(("grp", "sp"), "tp"),
        P(("grp", "sp"), "tp"),
        P(("grp", "sp")),
        P(None, "tp", None),
        P(None, "tp", None),
        P(None, "tp", None, None),
        P(None, "tp", None, None),
        P(None, "tp", None),
        P(None, "tp", None),
        P(None, "tp", None, None),
        P(None, "tp", None, None),
        P(None, "tp"),
        P(None, "tp"),
        P(None, "tp"),
        P(("grp", "sp"), "tp"),
        P("tp"),
        P("sp", "tp"),
        P("sp", "tp"),
        P(None, None, "tp"),
        P("tp", "sp"),
    )
    return jax.shard_map(
        functools.partial(on_device, mesh.shape["sp"], mesh.shape["tp"], mesh.shape["grp"]),
        mesh=mesh, in_specs=placed, out_specs=P(("grp", "sp"), "tp"), check_vma=False
    )
```

```python
import functools

import jax
import jax.numpy as jnp
from jax import lax
from jax.experimental import pallas as pl
from jax.experimental.pallas import tpu as pltpu
from jax.sharding import PartitionSpec as P

GROUP = 16
LANES = 128
epsilon = 1e-06
f32 = jnp.float32
bf16 = jnp.bfloat16


def sin_cos(angle):
    turns = jnp.round(angle * 0.6366197723675814)
    r = angle - turns * 1.5703125
    r = r - turns * 4.837512969970703125e-4
    r = r - turns * 7.54978995489188216e-8
    z = r * r
    s = ((-1.9515295891e-4 * z + 8.3321608736e-3) * z - 1.6666654611e-1) * z * r + r
    c = ((2.443315711809948e-5 * z - 1.388731625493765e-3) * z + 4.166664568298827e-2) * z * z - 0.5 * z + 1.0
    quadrant = turns.astype(jnp.int32)
    odd = (quadrant & 1) == 1
    sin = jnp.where(odd, c, s)
    cos = jnp.where(odd, s, c)
    sin = jnp.where((quadrant & 2) == 2, -sin, sin)
    cos = jnp.where(((quadrant + 1) & 2) == 2, -cos, cos)
    return sin, cos


def decay_of(rate, turn, span):
    shrink = jnp.exp(-rate * span)
    sin, cos = sin_cos(turn * span)
    return shrink * cos, shrink * sin


def times(ar, ai, br, bi):
    return ar * br - ai * bi, ar * bi + ai * br


def split(value):
    high = value.astype(bf16)
    return high, (value - high.astype(f32)).astype(bf16)


def dot(a, b):
    return jnp.dot(a, b, preferred_element_type=f32)


def dot_nt(a, b):
    return lax.dot_general(a, b, (((1,), (1,)), ((), ())), preferred_element_type=f32)


def packed(wide, narrow):
    wide = wide.reshape(-1, wide.shape[-1])
    narrow = narrow.reshape(-1, narrow.shape[-1])
    states, small = wide.shape[1] // 2, narrow.shape[1] // 2

    def zeros(like, lanes):
        return jnp.zeros((like.shape[0], lanes), f32)

    top = jnp.concatenate(
        [wide[:, :states], zeros(wide, LANES - states), wide[:, states:], zeros(wide, LANES - states)], axis=1)
    low = jnp.concatenate(
        [zeros(narrow, states), narrow[:, :small], zeros(narrow, LANES - small),
         narrow[:, small:], zeros(narrow, LANES - states - small)], axis=1)
    return jnp.concatenate([top, low], axis=0)


def kernel(
    n, nt, ng,
    spacing, xw_ref, xn_ref, rw_ref, tw_ref, rn_ref, tn_ref, dw_ref, dn_ref, rdw_ref, rdn_ref, skip_ref, ov_ref, og_ref, stream_ref, gain_ref,
    taps_ref, upv_ref, upg_ref, down_ref,
    out_ref,
    upv, upg, down, kick, dec, ends, mix, mid, gain, pre, part, near, got, own, sums, done,
    w_send, w_recv, w_local, y_send, y_recv, e_send, e_recv, g_send, g_recv, m_send, m_recv,
    z_send, z_recv, t_send, f_send, t_recv, d_send, d_recv, p_send, p_recv, s_send, s_recv,
):
    me, mt, mg = lax.axis_index("sp"), lax.axis_index("tp"), lax.axis_index("grp")
    partner = mt + 1 - 2 * lax.rem(mt, 2)
    side = nt // 2
    tokens, channels = xw_ref.shape
    groups = rw_ref.shape[1]
    width = upv.shape[1]
    rows = upv_ref.shape[0]
    cols = out_ref.shape[1]
    limit = upv_ref.shape[1] - width

    def remote(src, dst, send, recv, axis, peer):
        return pltpu.make_async_remote_copy(
            src_ref=src, dst_ref=dst, send_sem=send, recv_sem=recv,
            device_id={axis: peer}, device_id_type=pl.DeviceIdType.MESH)

    def start_of(index):
        return pl.multiple_of(jnp.minimum(index * width, limit), LANES)

    barrier = pltpu.get_barrier_semaphore()
    for offset in range(1, n):
        pl.semaphore_signal(barrier, inc=1, device_id={"sp": lax.rem(me + offset, n)},
                            device_id_type=pl.DeviceIdType.MESH)
    for offset in range(1, nt):
        pl.semaphore_signal(barrier, inc=1, device_id={"tp": lax.rem(mt + offset, nt)},
                            device_id_type=pl.DeviceIdType.MESH)
    for offset in range(1, ng):
        pl.semaphore_signal(barrier, inc=1, device_id={"grp": lax.rem(mg + offset, ng)},
                            device_id_type=pl.DeviceIdType.MESH)
    pl.semaphore_wait(barrier, n + nt + ng - 3)

    def weight_parts(which, target, slot, index, count):
        begin = start_of(target)
        full = width if which == 2 else rows
        size = full // count
        first_row = pl.multiple_of(index * size, size)
        if which == 2:
            return (down_ref.at[pl.ds(pl.multiple_of(begin + first_row, GROUP), size), :],
                    down.at[slot, pl.ds(first_row, size), :])
        source, held = ((upv_ref, upv), (upg_ref, upg))[which]
        return (source.at[pl.ds(first_row, size), pl.ds(begin, width)],
                held.at[pl.ds(pl.multiple_of(slot * rows + first_row, size), size), :])

    def weight_copy(which, target, slot):
        src, dst = weight_parts(which, target, slot, mg, ng)
        return remote(src, dst, w_send.at[which, target], w_recv.at[which, slot], "sp", target)

    def share_copy(which, slot, index):
        _, block = weight_parts(which, me, slot, index, ng)
        offset = 1 if index is mg else 0
        return remote(block, block, y_send.at[which, slot], y_recv.at[which, slot], "grp",
                      lax.rem(mg + offset, ng))

    def weight_share(which):
        for offset in range(1, n):
            peer = lax.rem(me + offset, n)
            weight_copy(which, me, peer).wait_recv()
            if ng == 2:
                share_copy(which, peer, mg).start()

    def weight_start(which):
        for offset in range(1, n):
            weight_copy(which, lax.rem(me + offset, n), me).start()

    def weight_wait(which):
        for offset in range(1, n):
            peer = lax.rem(me + offset, n)
            weight_copy(which, peer, me).wait_send()
            if ng == 2:
                share_copy(which, peer, mg).wait_send()
                share_copy(which, peer, 1 - mg).wait_recv()
        src, dst = weight_parts(which, me, me, 0, 1)
        pltpu.make_async_copy(src, dst, w_local.at[which]).wait()

    weight_start(0)
    for which in range(3):
        src, dst = weight_parts(which, me, me, 0, 1)
        pltpu.make_async_copy(src, dst, w_local.at[which]).start()

    def gain_copy(target, slot):
        return remote(gain_ref, gain.at[slot], g_send.at[target], g_recv.at[slot], "tp", target)

    for offset in range(1, nt):
        gain_copy(lax.rem(mt + offset, nt), mt).start()
    gain[mt] = gain_ref[...]

    x = jnp.concatenate([xw_ref[...], xn_ref[...]], axis=1)
    rest = jnp.ones((groups, LANES - rw_ref.shape[2] - rn_ref.shape[2]), f32)
    lane_group = lax.rem(lax.broadcasted_iota(jnp.int32, x.shape, 1), channels) // GROUP
    for d in range(2):
        high, low = split(packed(dw_ref[d], dn_ref[d]))
        for g in range(groups):
            picked = jnp.where(lane_group == g, x, jnp.zeros_like(x))
            pushed = dot(picked, high) + dot(picked, low)
            place = pl.ds(g, tokens, stride=groups)
            kick[d, 0, place, :] = pushed[:, :LANES]
            kick[d, 1, place, :] = pushed[:, LANES:]

    rates = [jnp.concatenate([rw_ref[d], rn_ref[d], rest], axis=1) for d in range(2)]
    turns = [jnp.concatenate([tw_ref[d], tn_ref[d], rest], axis=1) for d in range(2)]
    inverse = []
    for d in range(2):
        square = rates[d] * rates[d] + turns[d] * turns[d]
        inverse.append((-rates[d] / square, -turns[d] / square))

    def spot(d, i):
        return i if d == 0 else tokens - 1 - i

    def first(i, carry):
        state, total = list(carry[:4]), carry[4]
        for d in range(2):
            t = spot(d, i)
            step = spacing[t]
            if d == 0:
                total = total + step
            place = pl.ds(pl.multiple_of(t * groups, groups), groups)
            dr, di = decay_of(rates[d], turns[d], step)
            cr, ci = times(dr - 1.0, di, *inverse[d])
            kr, ki = times(cr, ci, kick[d, 0, place, :], kick[d, 1, place, :])
            dec[d, 0, place, :] = dr
            dec[d, 1, place, :] = di
            kick[d, 0, place, :] = kr
            kick[d, 1, place, :] = ki
            ar, ai = times(dr, di, state[2 * d], state[2 * d + 1])
            state[2 * d], state[2 * d + 1] = ar + kr, ai + ki
        return (*state, total)

    zero = jnp.zeros((groups, LANES), f32)
    found = lax.fori_loop(0, tokens, first, (zero, zero, zero, zero, jnp.float32(0.0)), unroll=4)
    last_lane = lax.broadcasted_iota(jnp.int32, zero.shape, 1) == LANES - 1
    for d in range(2):
        ends[me, d, 0] = jnp.where(last_lane, found[4], found[2 * d])
        ends[me, d, 1] = found[2 * d + 1]

    def ends_copy(target, slot):
        d = jnp.where(target > slot, 0, 1)
        return remote(ends.at[slot, d], ends.at[slot, d], e_send.at[target], e_recv.at[slot], "sp", target)

    for offset in range(1, n):
        ends_copy(lax.rem(me + offset, n), me).start()
    weight_start(1)
    for offset in range(1, n):
        peer = lax.rem(me + offset, n)
        ends_copy(peer, me).wait_send()
        ends_copy(me, peer).wait_recv()

    carry = []
    for d in range(2):
        cr, ci = zero, zero
        for k in range(n):
            s = k if d == 0 else n - 1 - k
            use = (s < me) if d == 0 else (s > me)
            nr, ni = times(*decay_of(rates[d], turns[d], ends[s, d, 0][:, LANES - 1:]), cr, ci)
            flag = jnp.where(use, 1, 0)
            keep = jnp.full((groups, LANES), flag, jnp.int32) == 1
            cr = jnp.where(keep, nr + ends[s, d, 0], cr)
            ci = jnp.where(keep, ni + ends[s, d, 1], ci)
        carry += [cr, ci]
    weight_share(0)

    def second(i, carry):
        state = list(carry)
        for d in range(2):
            t = spot(d, i)
            place = pl.ds(pl.multiple_of(t * groups, groups), groups)
            ar, ai = times(dec[d, 0, place, :], dec[d, 1, place, :], state[2 * d], state[2 * d + 1])
            state[2 * d] = ar + kick[d, 0, place, :]
            state[2 * d + 1] = ai + kick[d, 1, place, :]
            kick[d, 0, place, :] = state[2 * d]
            kick[d, 1, place, :] = state[2 * d + 1]
        return tuple(state)

    lax.fori_loop(0, tokens, second, tuple(carry), unroll=4)

    reading = jnp.concatenate([skip_ref[0:1, :], skip_ref[1:2, :]], axis=1) * x.astype(f32)
    for d in range(2):
        high, low = split(packed(rdw_ref[d], rdn_ref[d]))
        for g in range(groups):
            place = pl.ds(g, tokens, stride=groups)
            state = jnp.concatenate([kick[d, 0, place, :], kick[d, 1, place, :]], axis=1)
            state_high, state_low = split(state)
            value = dot_nt(state_high, high) + dot_nt(state_low, high) + dot_nt(state_high, low)
            reading = reading + jnp.where(lane_group == g, value, 0.0)
    mix[mt] = jax.nn.gelu(reading).astype(bf16)

    def mix_copy(target, slot):
        return remote(mix.at[slot], mix.at[slot], m_send.at[target], m_recv.at[slot], "tp", target)

    for offset in range(1, nt):
        mix_copy(lax.rem(mt + offset, nt), mt).start()
    weight_start(2)
    for offset in range(1, nt):
        peer = lax.rem(mt + offset, nt)
        mix_copy(peer, mt).wait_send()
        mix_copy(mt, peer).wait_recv()

    weight_share(1)
    value = jnp.zeros((tokens, cols), f32)
    gate = jnp.zeros((tokens, cols), f32)
    half = ov_ref.shape[0] // 2
    for k in range(nt):
        for h in range(2):
            piece = mix[k][:, h * channels:(h + 1) * channels]
            at = slice(h * half + k * channels, h * half + (k + 1) * channels)
            value = value + dot(piece, ov_ref[at, :])
            gate = gate + dot(piece, og_ref[at, :])
    mid[me, mt] = (stream_ref[...].astype(f32) + value * jax.nn.sigmoid(gate)).astype(bf16)

    def z_copy(target, slot):
        return remote(mid.at[slot, mt], mid.at[slot, mt], z_send.at[target], z_recv.at[slot], "sp", target)

    def t_copy(s, target, slot):
        return remote(mid.at[s, slot], mid.at[s, slot], t_send.at[s, target], t_recv.at[s, slot], "tp", target)

    def f_copy(s, slot):
        return remote(mid.at[s, slot], mid.at[s, slot], f_send.at[s, slot], t_recv.at[s, slot], "tp", partner)

    def spread(s):
        for offset in range(1, side):
            t_copy(s, lax.rem(mt + 2 * offset, nt), mt).start()
        f_copy(s, mt).start()

    def relay(s):
        for offset in range(1, side):
            peer = lax.rem(mt + 2 * offset, nt)
            t_copy(s, mt, peer).wait_recv()
            f_copy(s, peer).start()

    for offset in range(1, n):
        z_copy(lax.rem(me + offset, n), me).start()
    spread(me)
    for offset in range(1, nt):
        peer = lax.rem(mt + offset, nt)
        gain_copy(peer, mt).wait_send()
        gain_copy(mt, peer).wait_recv()
    for i in range(2):
        pre[pl.ds(i * (8 + n * tokens), 8), :] = jnp.zeros((8, 2 * width), f32)
    weight_share(2)
    relay(me)
    weight_wait(0)
    weight_wait(1)

    def raise_block(s):
        for offset in range(side):
            peer = lax.rem(mt + 2 * offset, nt)
            if offset:
                t_copy(s, peer, mt).wait_send()
            f_copy(s, peer).wait_send()
            f_copy(s, lax.rem(partner + 2 * offset, nt)).wait_recv()
        squares = jnp.zeros((tokens, 1), f32)
        for k in range(nt):
            piece = mid[s, k].astype(f32)
            squares = squares + jnp.sum(piece * piece, axis=1, keepdims=True)
        scale = lax.rsqrt(squares / (nt * cols) + epsilon)
        normed = jnp.concatenate(
            [(mid[s, k].astype(f32) * scale * gain[k]).astype(bf16) for k in range(nt)], axis=1)
        place = pl.ds(pl.multiple_of(8 + s * tokens, 8), tokens)
        pre[place, :width] = dot(normed, upv[...]).astype(bf16).astype(f32)
        pre[place, width:] = dot(normed, upg[...]).astype(bf16).astype(f32)

    for offset in range(1, n):
        peer = lax.rem(me + offset, n)
        z_copy(me, peer).wait_recv()
        spread(peer)
        raise_block(lax.rem(me + offset - 1, n))
        relay(peer)
    raise_block(lax.rem(me + n - 1, n))
    for offset in range(1, n):
        z_copy(lax.rem(me + offset, n), me).wait_send()

    weight_wait(2)
    begin = start_of(me)
    own_from = me * width - begin
    valid = lax.broadcasted_iota(jnp.int32, (1, width), 1) >= own_from

    def conv_of(k, s):
        base = pl.multiple_of(s * tokens, 8)
        block = pre[pl.ds(base, tokens + 16), k * width:(k + 1) * width]
        tap = taps_ref[k, :, pl.ds(begin, width)]
        return (tap[0:1] * block[7:7 + tokens] + tap[1:2] * block[8:8 + tokens]
                + tap[2:3] * block[9:9 + tokens])

    def d_copy(s, target):
        return remote(part.at[s, target], near.at[s, target], d_send.at[s, target], d_recv.at[s, target],
                      "tp", partner)

    def p_copy(s, target, slot):
        return remote(part.at[s, target], got.at[s, slot], p_send.at[s, target], p_recv.at[s, slot],
                      "tp", target)

    def pass_on(s):
        for offset in range(side):
            target = lax.rem(mt + 2 * offset, nt)
            d_copy(s, target).wait_recv()
            total = part[s, target].astype(f32) + near[s, target].astype(f32)
            if offset:
                part[s, target] = total.astype(bf16)
                p_copy(s, target, mt).start()
            else:
                own[s] = total

    for step in range(n):
        s = lax.rem(me + 1 + step, n)
        conv_value, conv_gate = conv_of(0, s), conv_of(1, s)
        hidden = conv_gate * jax.nn.sigmoid(conv_gate) * conv_value
        hidden = jnp.where(valid, hidden, 0.0).astype(bf16)
        per = down.shape[2]
        for k in range(n):
            terms = dot(hidden, down[k]).astype(bf16)
            if per >= cols:
                for j in range(per // cols):
                    part[s, k * (per // cols) + j] = terms[:, j * cols:(j + 1) * cols]
            else:
                ratio = cols // per
                part[s, k // ratio, :, (k % ratio) * per:(k % ratio + 1) * per] = terms
        for offset in range(side):
            d_copy(s, lax.rem(partner + 2 * offset, nt)).start()
        if step:
            pass_on(lax.rem(me + step, n))
    pass_on(me)

    def s_copy(target, slot):
        return remote(sums.at[target], done.at[slot], s_send.at[target], s_recv.at[slot], "sp", target)

    for step in range(n):
        s = lax.rem(me + 1 + step, n)
        total = own[s]
        for offset in range(side):
            d_copy(s, lax.rem(partner + 2 * offset, nt)).wait_send()
            if offset:
                peer = lax.rem(mt + 2 * offset, nt)
                p_copy(s, peer, mt).wait_send()
                p_copy(s, mt, peer).wait_recv()
                total = total + got[s, peer].astype(f32)
        if step < n - 1:
            sums[s] = total.astype(bf16)
            s_copy(s, me).start()
    for offset in range(1, n):
        peer = lax.rem(me + offset, n)
        s_copy(peer, me).wait_send()
        s_copy(me, peer).wait_recv()
        total = total + done[peer].astype(f32)
    out_ref[...] = (mid[me, mt].astype(f32) + total).astype(bf16)


def on_device(
    n, nt, ng,
    input_wide, input_narrow, spacing, rate_wide, turn_wide, drive_wide, read_wide,
    narrow_decay_rate, turn_narrow, drive_narrow, read_narrow, skip_gain, out_value, out_gate,
    stream, norm_gain, up_value, up_gate, conv_taps, down_weight,
):
    tokens = spacing.shape[0]
    groups = rate_wide.shape[1]
    extra = -up_value.shape[1] % LANES
    if extra:
        up_value = jnp.pad(up_value, ((0, 0), (0, extra)))
        up_gate = jnp.pad(up_gate, ((0, 0), (0, extra)))
        conv_taps = jnp.pad(conv_taps, ((0, 0), (0, 0), (0, extra)))
        down_weight = jnp.pad(down_weight, ((0, extra), (0, 0)))
    hidden = up_value.shape[1]
    width = -(-hidden // (n * LANES)) * LANES
    rows = up_value.shape[0]
    cols = stream.shape[1]
    per = down_weight.shape[1]
    vmem = pl.BlockSpec(memory_space=pltpu.VMEM)
    anywhere = pl.BlockSpec(memory_space=pl.ANY)
    dma = pltpu.SemaphoreType.DMA
    return pl.pallas_call(
        functools.partial(kernel, n, nt, ng),
        out_shape=jax.ShapeDtypeStruct((tokens, cols), bf16),
        in_specs=[pl.BlockSpec(memory_space=pltpu.SMEM)] + [vmem] * 16 + [anywhere] * 3,
        out_specs=vmem,
        scratch_shapes=[
            pltpu.VMEM((rows * n, width), bf16),
            pltpu.VMEM((rows * n, width), bf16),
            pltpu.VMEM((n, width, per), bf16),
            pltpu.VMEM((2, 2, tokens * groups, LANES), f32),
            pltpu.VMEM((2, 2, tokens * groups, LANES), f32),
            pltpu.VMEM((n, 2, 2, groups, LANES), f32),
            pltpu.VMEM((nt, tokens, 2 * input_wide.shape[1]), bf16),
            pltpu.VMEM((n, nt, tokens, cols), bf16),
            pltpu.VMEM((nt, 1, cols), f32),
            pltpu.VMEM((n * tokens + 16, 2 * width), f32),
            pltpu.VMEM((n, nt, tokens, cols), bf16),
            pltpu.VMEM((n, nt, tokens, cols), bf16),
            pltpu.VMEM((n, nt, tokens, cols), bf16),
            pltpu.VMEM((n, tokens, cols), f32),
            pltpu.VMEM((n, tokens, cols), bf16),
            pltpu.VMEM((n, tokens, cols), bf16),
            dma((3, n)), dma((3, n)), dma((3,)), dma((3, n)), dma((3, n)),
            dma((n,)), dma((n,)),
            dma((nt,)), dma((nt,)),
            dma((nt,)), dma((nt,)),
            dma((n,)), dma((n,)),
            dma((n, nt)), dma((n, nt)), dma((n, nt)),
            dma((n, nt)), dma((n, nt)),
            dma((n, nt)), dma((n, nt)),
            dma((n,)), dma((n,)),
        ],
        compiler_params=pltpu.CompilerParams(
            collective_id=0, has_side_effects=True, vmem_limit_bytes=60 * 1024 * 1024),
    )(spacing, input_wide, input_narrow, rate_wide, turn_wide, narrow_decay_rate, turn_narrow,
      drive_wide, drive_narrow, read_wide, read_narrow, skip_gain, out_value, out_gate, stream, norm_gain.reshape(1, -1),
      conv_taps, up_value, up_gate, down_weight)


def solution(mesh):
    placed = (
        P(("grp", "sp"), "tp"),
        P(("grp", "sp"), "tp"),
        P(("grp", "sp")),
        P(None, "tp", None),
        P(None, "tp", None),
        P(None, "tp", None, None),
        P(None, "tp", None, None),
        P(None, "tp", None),
        P(None, "tp", None),
        P(None, "tp", None, None),
        P(None, "tp", None, None),
        P(None, "tp"),
        P(None, "tp"),
        P(None, "tp"),
        P(("grp", "sp"), "tp"),
        P("tp"),
        P("sp", "tp"),
        P("sp", "tp"),
        P(None, None, "tp"),
        P("tp", "sp"),
    )
    return jax.shard_map(
        functools.partial(on_device, mesh.shape["sp"], mesh.shape["tp"], mesh.shape["grp"]),
        mesh=mesh, in_specs=placed, out_specs=P(("grp", "sp"), "tp"), check_vma=False
    )
```
